32 devices in a mesh: fs: 8 (over z, x), tp: 4 (over y, core).
Axes of the slice: x: 2, y: 2, z: 4, core: 2. Of those that a mesh axis runs over, the one named last changes fastest.
Arguments:
- tokens: bfloat16 [8192, 2048], P(('fs', 'tp')), may hold values from -130 to 130
- pool_weight: bfloat16 [4, 512, 512], P(None, 'fs'), may hold values from -0.25 to 0.25
- pool_scale: float32 [2048], replicated, may hold values from 0.5 to 1.5
- gain_mix: float32 [2048], replicated, may hold values from 0.1 to 1.9
- gain_mlp: float32 [2048], replicated, may hold values from 0.1 to 1.9
- w_up: bfloat16 [8192, 2048], P('tp', 'fs'), may hold values from -0.125 to 0.125
- w_down: bfloat16 [8192, 2048], P('tp', 'fs'), may hold values from -0.0625 to 0.0625
- gain_out: float32 [2048], P('tp'), may hold values from 0.1 to 1.9
Outputs:
- result: bfloat16 [8192, 2048], P('fs', 'tp')
The draws below stay inside these ranges and needn't reach their ends.
All inputs are finite; a program needn't handle non-finite values.
Results may differ from the reference program's by a relative error of at most 0.013.
Values may be sent and summed in bfloat16 or wider, within the bound.
A program may use at most 64 MiB of HBM per device.

```python
import math
import jax
import jax.numpy as jnp
from jax import lax

D = 2048
FF = 8192
GROUP = 512
SEQ_LEN = 1024
TOKENS = 8192
N_TP = 4


def draw_tokens(key, part):
    key_row, key_col, key_base = jax.random.split(jax.random.fold_in(key, 11), 3)
    column = jnp.arange(D, dtype=jnp.float32) / D
    row_scale = jnp.exp(jax.random.uniform(key_row, (TOKENS, 1), jnp.float32, math.log(0.5), math.log(5.0)))
    col_scale = jnp.exp(jax.random.uniform(key_col, (1, D), jnp.float32, math.log(0.4), math.log(2.5)))
    base = jnp.clip(jax.random.normal(key_base, (TOKENS, D), jnp.float32), -4.0, 4.0)
    trend = 3.0 ** (0.5 * column)
    return (base * row_scale * col_scale * trend[None, :]).astype(jnp.bfloat16)


def steps_of(key, dims, shards, least, largest):
    factor_of, own = 1.0, jax.random.fold_in(key, 6)
    for dim, shards_of in shards:
        heights = jnp.exp(jax.random.uniform(jax.random.fold_in(own, dim), (shards_of,), jnp.float32, least / len(shards), largest / len(shards)))
        factor_of = factor_of * jnp.repeat(heights, dims[dim] // shards_of).reshape([-1 if axis == dim else 1 for axis in range(len(dims))])
    return factor_of


def centred(stream_key, extent, spread, most, cuts=(), kind=jnp.bfloat16):
    level = steps_of(stream_key, extent, cuts, -0.22, 0.18) if cuts else 1.0
    drawn = jax.random.normal(stream_key, extent, jnp.float32) * spread * level
    return jnp.minimum(jnp.maximum(drawn, -most), most).astype(kind)


def setup_inputs(seed: int = 0) -> dict:
    arg_keys = jax.random.split(jax.random.key(seed), 9)
    tokens = draw_tokens(jax.random.fold_in(arg_keys[8], 71), 0)
    pool_weight = centred(arg_keys[1], (4, GROUP, GROUP), GROUP ** -0.5, 0.25, ((1, 8),))
    pool_scale = jnp.clip(jax.random.uniform(arg_keys[2], (D,), jnp.float32, 0.5, 1.5), 0.5, 1.5)
    gain_mix = jnp.clip(1.0 + 0.18 * jax.random.normal(arg_keys[3], (D,), jnp.float32), 0.1, 1.9)
    gain_mlp = jnp.clip(1.0 + 0.18 * jax.random.normal(arg_keys[4], (D,), jnp.float32), 0.1, 1.9)
    w_up = centred(arg_keys[5], (FF, D), D ** -0.5, 0.125, ((0, 4), (1, 8)))
    w_down = centred(arg_keys[6], (FF, D), FF ** -0.5, 0.0625, ((0, 4), (1, 8)))
    gain_out = jnp.clip(1.0 + 0.18 * jax.random.normal(arg_keys[7], (D,), jnp.float32), 0.1, 1.9)
    return dict(tokens=tokens, pool_weight=pool_weight, pool_scale=pool_scale, gain_mix=gain_mix, gain_mlp=gain_mlp, w_up=w_up, w_down=w_down, gain_out=gain_out)


EPS = 1e-06
WINDOWS = (2, 4, 8, 16)

def rms_scale(values, gain):
    return values * lax.rsqrt(lax.optimization_barrier(jnp.mean(values * values, axis=-1, keepdims=True)) + EPS) * gain

def window_mean(values, reach):
    cumulative = jnp.concatenate([jnp.zeros_like(values[:, :1]), jnp.cumsum(values, axis=1)], axis=1)
    position = jnp.arange(SEQ_LEN, dtype=jnp.int32)
    lower = jnp.clip(position - reach // 2, 0, SEQ_LEN).astype(jnp.int32)
    upper = jnp.clip(position + reach // 2, 0, SEQ_LEN).astype(jnp.int32)
    sums = jnp.take(cumulative, upper, axis=1) - jnp.take(cumulative, lower, axis=1)
    counts = (upper - lower).astype(jnp.float32)[None, :, None]
    return sums / counts

def reference(tokens, pool_weight, pool_scale, gain_mix, gain_mlp, w_up, w_down, gain_out):
    inputs = tokens.astype(jnp.float32)
    normed = rms_scale(inputs, gain_mix).astype(jnp.bfloat16)
    normed_seq = normed.astype(jnp.float32).reshape(-1, SEQ_LEN, D)
    pieces = []
    for index, reach in enumerate(WINDOWS):
        part = normed_seq[..., index * GROUP:(index + 1) * GROUP]
        pooled = (window_mean(part, reach) - part).astype(jnp.bfloat16).reshape(-1, GROUP)
        pieces.append(jnp.dot(pooled, pool_weight[index], preferred_element_type=jnp.float32))
    mixed = jnp.concatenate(pieces, axis=1) * pool_scale
    first_sum = (inputs + mixed).astype(jnp.bfloat16)
    first_f32 = first_sum.astype(jnp.float32)
    inner = rms_scale(first_f32, gain_mlp).astype(jnp.bfloat16)
    block = FF // N_TP

    def add_block(index, total):
        begin = (index * block).astype(jnp.int32)
        up_block = lax.dynamic_slice_in_dim(w_up, begin, block, 0)
        down_block = lax.dynamic_slice_in_dim(w_down, begin, block, 0)
        pre = jnp.dot(inner, up_block.T, preferred_element_type=jnp.float32)
        hidden = jnp.square(jax.nn.relu(pre)).astype(jnp.bfloat16)
        partial_sum = jnp.dot(hidden, down_block, preferred_element_type=jnp.float32).astype(jnp.bfloat16)
        partial_sum = lax.optimization_barrier(partial_sum)
        return total + partial_sum.astype(jnp.float32)
    channel_out = lax.fori_loop(jnp.int32(0), jnp.int32(N_TP), add_block, jnp.zeros((tokens.shape[0], D), jnp.float32))
    second_sum = first_f32 + channel_out
    return rms_scale(second_sum, gain_out).astype(jnp.bfloat16)
```

```python
import functools

import jax
import jax.numpy as jnp
from jax import lax
from jax.experimental import pallas as pl
from jax.experimental.pallas import tpu as pltpu
from jax.sharding import PartitionSpec as P

SEQ_LEN = 1024
EPS = 1e-06
WINDOWS = (2, 4, 8, 16)
HALO = 16
MESH = pl.DeviceIdType.MESH
POOL, UP, DOWN = 0, 1, 2


def ring_order(n, nx):
    nz = n // nx
    if nx < 2 or nz < 2 or nz % 2:
        return list(range(n))
    order = []
    for z in range(nz):
        xs = list(range(1, nx))
        order += [z * nx + x for x in (xs if z % 2 == 0 else xs[::-1])]
    return order + [z * nx for z in range(nz - 1, -1, -1)]


def lookup(table, index):
    value = jnp.int32(table[0])
    for i in range(1, len(table)):
        value = jnp.where(index == i, jnp.int32(table[i]), value)
    return value


def ring_kernel(
    n, tp, order, tok_ref, pool_ref, up_ref, down_ref, scale_ref, gmix_ref, gmlp_ref,
    gout_ref, out_ref,
    pool_full, up_full, down_full, ext, first, inner_all, hidden, fcols, blocks, parts,
    before, after, edge, total, stat, stat_out, stat_in,
    ring_send, ring_recv, in_send, in_recv, fc_send, fc_recv, halo_send, halo_recv, rs_send, rs_recv,
    pair_send, pair_recv, st_send, st_recv,
):
    rows, width = tok_ref.shape
    group = width // 4
    hid, cols = up_ref.shape
    depth = pool_ref.shape[1]
    own_cols = width // tp
    per = n // tp
    seq = rows * tp
    me_fs, me = lax.axis_index("fs"), lax.axis_index("tp")
    place_of = [order.index(i) for i in range(n)]
    place = lookup(place_of, me_fs)

    def at(offset):
        return lookup(order, lax.rem(place + offset + 2 * n, n))

    owners = {0: me_fs}
    for d in range(1, n // 2 + 1):
        owners[d] = at(d)
        owners[-d] = at(-d)
    right, left = owners[1], owners[-1]

    barrier = pltpu.get_barrier_semaphore()
    for peer in (right, left):
        pl.semaphore_signal(barrier, inc=1, device_id={"fs": peer, "tp": me}, device_id_type=MESH)
    for d in range(1, tp):
        pl.semaphore_signal(
            barrier, inc=1, device_id={"fs": me_fs, "tp": lax.rem(me + d, tp)}, device_id_type=MESH
        )
    pl.semaphore_wait(barrier, 2 + tp - 1)

    hops = n // 2
    cores = 2 if tp % 2 == 0 else 1
    core = lax.rem(me, cores)
    lanes = 2 if cols % 256 == 0 else 1
    fine = cols // lanes

    def view(stream, full, owner, piece, sub=None):
        if stream == POOL:
            ref = pool_full if full else pool_ref
            half = ref.shape[0] // (2 * cores)
            r = pl.ds(pl.multiple_of(owner * depth, depth), depth) if full else slice(None)
            return ref.at[pl.ds((core * 2 + piece) * half, half), r, :]
        ref = (up_full if full else up_ref) if stream == UP else (down_full if full else down_ref)
        half = hid // 2
        c = pl.ds(pl.multiple_of(owner * cols, cols), cols) if full else slice(None)
        if sub is not None:
            c = pl.ds(pl.multiple_of(owner * cols + sub * fine, fine), fine)
        return ref.at[pl.ds(piece * half, half), c]

    def count(side, piece):
        return hops if piece == side else hops - 1

    def slot(stream, side, piece, hop, sub):
        if sub:
            return 12 * hops + side * (lanes - 1) + sub - 1
        return ((stream * 2 + side) * 2 + piece) * hops + hop

    def subs(stream, hop):
        return range(lanes) if stream == DOWN and hop == hops - 1 and hop > 0 else (None,)

    def ring(stream, side, piece, hop, sub):
        owner = owners[-hop] if side == 0 else owners[hop]
        return pltpu.make_async_remote_copy(
            src_ref=view(stream, hop > 0, owner, piece, sub),
            dst_ref=view(stream, True, owner, piece, sub),
            send_sem=ring_send.at[slot(stream, side, piece, hop, sub)],
            recv_sem=ring_recv.at[slot(stream, side, piece, hop, sub)],
            device_id={"fs": right if side == 0 else left, "tp": me},
            device_id_type=MESH,
        )

    started = []

    def arrived(stream, side, piece, hop, sub=None):
        owner = owners[-hop - 1] if side == 0 else owners[hop + 1]
        pltpu.make_async_remote_copy(
            src_ref=view(stream, True, owner, piece, sub),
            dst_ref=view(stream, True, owner, piece, sub),
            send_sem=ring_send.at[slot(stream, side, piece, hop, sub)],
            recv_sem=ring_recv.at[slot(stream, side, piece, hop, sub)],
            device_id={"fs": right if side == 0 else left, "tp": me},
            device_id_type=MESH,
        ).wait_recv()

    def start(stream, hop, which=(0, 1)):
        for w in which:
            for side in (0, 1):
                piece = side if w == 0 else 1 - side
                if hop < count(side, piece):
                    if hop > 0:
                        arrived(stream, side, piece, hop - 1)
                    for sub in subs(stream, hop):
                        copy = ring(stream, side, piece, hop, sub)
                        copy.start()
                        started.append(copy)

    def finish(stream, sub=None):
        for side in (0, 1):
            arrived(stream, side, side, hops - 1, sub)

    def settle(stream, hop):
        if hop == hops - 2:
            for side in (0, 1):
                arrived(stream, side, 1 - side, hop)

    start(POOL, 0)
    start(UP, 0, (0,))

    step = 32 if rows % 32 == 0 else rows

    @pl.loop(0, rows // step)
    def _(i):
        r = pl.ds(pl.multiple_of(i * step, step), step)
        x = tok_ref[r, :].astype(jnp.float32)
        y = x * lax.rsqrt(jnp.mean(x * x, axis=-1, keepdims=True) + EPS) * gmix_ref[...]
        y = y.astype(jnp.bfloat16)
        ext[pl.ds(pl.multiple_of(HALO + i * step, HALO), step), :] = y.astype(jnp.float32)

    edge[0] = ext[rows : rows + HALO, :].astype(jnp.bfloat16)
    edge[1] = ext[HALO : 2 * HALO, :].astype(jnp.bfloat16)
    halos = []
    for side, (buffer, d) in enumerate(((before, 1), (after, tp - 1))):
        copy = pltpu.make_async_remote_copy(
            src_ref=edge.at[side],
            dst_ref=buffer,
            send_sem=halo_send.at[side],
            recv_sem=halo_recv.at[side],
            device_id={"fs": me_fs, "tp": lax.rem(me + d, tp)},
            device_id_type=MESH,
        )
        copy.start()
        halos.append(copy)

    start(POOL, 1)
    start(UP, 0, (1,))
    for hop in range(2, hops):
        start(POOL, hop)
    share = pl.ds(core * (pool_full.shape[0] // cores), pool_full.shape[0] // cores)
    pool_full[share, pl.ds(pl.multiple_of(me_fs * depth, depth), depth), :] = pool_ref[share, :, :]
    mine = pl.ds(pl.multiple_of(me_fs * cols, cols), cols)
    up_full[:, mine] = up_ref[...]
    down_full[:, mine] = down_ref[...]
    for copy in halos:
        copy.wait()
    offset = me * rows
    lower_open = (lax.rem(offset, SEQ_LEN) != 0).astype(jnp.float32)
    upper_open = (lax.rem(offset + rows, SEQ_LEN) != 0).astype(jnp.float32)
    ext[0:HALO, :] = before[...].astype(jnp.float32) * lower_open
    ext[rows + HALO : rows + 2 * HALO, :] = after[...].astype(jnp.float32) * upper_open
    start(UP, 1)
    settle(POOL, hops - 2)
    finish(POOL)
    if cores > 1:
        swap = pltpu.make_async_remote_copy(
            src_ref=pool_full.at[share],
            dst_ref=pool_full.at[share],
            send_sem=pair_send,
            recv_sem=pair_recv,
            device_id={"fs": me_fs, "tp": me + 1 - 2 * core},
            device_id_type=MESH,
        )
        swap.start()
        other = pl.ds((1 - core) * (pool_full.shape[0] // cores), pool_full.shape[0] // cores)
        pltpu.make_async_remote_copy(
            src_ref=pool_full.at[other],
            dst_ref=pool_full.at[other],
            send_sem=pair_send,
            recv_sem=pair_recv,
            device_id={"fs": me_fs, "tp": me + 1 - 2 * core},
            device_id_type=MESH,
        ).wait_recv()

    position = lax.rem(offset + lax.broadcasted_iota(jnp.int32, (rows, 1), 0), SEQ_LEN)
    for index, reach in enumerate(WINDOWS):
        half = reach // 2
        c = slice(index * group, (index + 1) * group)
        level = ext[:, c]
        own = level[HALO : HALO + rows]
        shift = 1
        while shift < reach:
            level = level + pltpu.roll(level, shift, 0)
            shift *= 2
        if half > 1:
            level = pltpu.roll(level, rows + 2 * HALO - (half - 1), 0)
        window = level[HALO : HALO + rows]
        counts = (jnp.minimum(position + half, SEQ_LEN) - jnp.maximum(position - half, 0)).astype(jnp.float32)
        pooled = (window / counts - own).astype(jnp.bfloat16)
        mixed = jnp.dot(pooled, pool_full[index], preferred_element_type=jnp.float32)
        first[:, c] = (tok_ref[:, c].astype(jnp.float32) + mixed * scale_ref[:, c]).astype(jnp.bfloat16)
    for hop in range(2, 3):
        if hop < hops:
            start(UP, hop)

    @pl.loop(0, rows // step)
    def _(i):
        r = pl.ds(pl.multiple_of(i * step, step), step)
        x = first[r, :].astype(jnp.float32)
        y = x * lax.rsqrt(jnp.mean(x * x, axis=-1, keepdims=True) + EPS) * gmlp_ref[...]
        inner_all[pl.ds(pl.multiple_of(me * rows + i * step, step), step), :] = y.astype(jnp.bfloat16)

    my_rows = pl.ds(pl.multiple_of(me * rows, rows), rows)
    inners, firsts = [], []
    for d in range(1, tp):
        peer = lax.rem(me + d, tp)
        copy = pltpu.make_async_remote_copy(
            src_ref=inner_all.at[my_rows, :],
            dst_ref=inner_all.at[my_rows, :],
            send_sem=in_send.at[d],
            recv_sem=in_recv.at[d],
            device_id={"fs": me_fs, "tp": peer},
            device_id_type=MESH,
        )
        copy.start()
        inners.append(copy)
    for d in range(1, tp):
        peer = lax.rem(me + d, tp)
        copy = pltpu.make_async_remote_copy(
            src_ref=first.at[:, pl.ds(pl.multiple_of(peer * own_cols, own_cols), own_cols)],
            dst_ref=fcols.at[my_rows, :],
            send_sem=fc_send.at[d],
            recv_sem=fc_recv.at[d],
            device_id={"fs": me_fs, "tp": peer},
            device_id_type=MESH,
        )
        copy.start()
        firsts.append(copy)
    fcols[my_rows, :] = first[:, pl.ds(pl.multiple_of(me * own_cols, own_cols), own_cols)]

    for hop in range(3, hops):
        start(UP, hop)
    settle(UP, hops - 2)
    start(DOWN, 0)
    finish(UP)
    for d in range(1, tp):
        source = pl.ds(pl.multiple_of(lax.rem(me + tp - d, tp) * rows, rows), rows)
        pltpu.make_async_remote_copy(
            src_ref=inner_all.at[source, :],
            dst_ref=inner_all.at[source, :],
            send_sem=in_send.at[d],
            recv_sem=in_recv.at[d],
            device_id={"fs": me_fs, "tp": lax.rem(me + d, tp)},
            device_id_type=MESH,
        ).wait_recv()

    tile = min(256, hid)

    @pl.loop(0, hid // tile)
    def _(j):
        h = pl.ds(pl.multiple_of(j * tile, tile), tile)
        pre = lax.dot_general(
            inner_all[...], up_full[h, :], (((1,), (1,)), ((), ())), preferred_element_type=jnp.float32
        )
        hidden[:, h] = jnp.square(jnp.maximum(pre, 0.0)).astype(jnp.bfloat16)

    sums = []
    part = min(512, seq)

    def block(k, owner, sub):
        c = pl.ds(pl.multiple_of(owner * cols + sub * fine, fine), fine)

        @pl.loop(0, seq // part)
        def _(i):
            r = pl.ds(pl.multiple_of(i * part, part), part)
            blocks[k, sub, r, :] = jnp.dot(
                hidden[r, :], down_full[:, c], preferred_element_type=jnp.float32
            ).astype(jnp.bfloat16)

        dest = owner // per
        d = lax.rem(dest - me + tp, tp)
        local = lax.rem(owner, per)
        copy = pltpu.make_async_remote_copy(
            src_ref=blocks.at[k, sub],
            dst_ref=parts.at[d, local, sub],
            send_sem=rs_send.at[k * lanes + sub],
            recv_sem=rs_recv.at[(d * per + local) * lanes + sub],
            device_id={"fs": me_fs, "tp": dest},
            device_id_type=MESH,
        )

        @pl.when(d == 0)
        def _():
            parts[0, local, sub] = blocks[k, sub]

        @pl.when(d != 0)
        def _():
            copy.start()

        sums.append((d, copy))

    def add_up(local, sub):
        for d in range(1, tp):
            pltpu.make_async_remote_copy(
                src_ref=blocks.at[0, sub],
                dst_ref=parts.at[d, local, sub],
                send_sem=rs_send.at[0],
                recv_sem=rs_recv.at[(d * per + local) * lanes + sub],
                device_id={"fs": me_fs, "tp": lax.rem(me + d, tp)},
                device_id_type=MESH,
            ).wait_recv()
        c = pl.ds(pl.multiple_of(local * cols + sub * fine, fine), fine)

        @pl.loop(0, seq // 128)
        def _(i):
            r = pl.ds(pl.multiple_of(i * 128, 128), 128)
            value = parts[0, local, sub, r, :].astype(jnp.float32)
            for d in range(1, tp):
                value = value + parts[d, local, sub, r, :].astype(jnp.float32)
            value = value + fcols[r, c].astype(jnp.float32)
            total[r, c] = value
            square = value * value
            lump = square[:, 0:128]
            for j in range(1, fine // 128):
                lump = lump + square[:, j * 128 : (j + 1) * 128]
            stat[r, :] = stat[r, :] + lump

    for sub in range(lanes):
        block(0, owners[0], sub)
    stat[...] = jnp.zeros_like(stat)
    k = 1
    for hop in range(1, hops):
        start(DOWN, hop)
        settle(DOWN, hop - 1)
        for owner in (owners[-hop], owners[hop]):
            for sub in range(lanes):
                block(k, owner, sub)
            k += 1
    for copy in firsts:
        copy.wait()
    last = lax.rem(owners[hops], per)
    for j in range(1, per):
        for sub in range(lanes):
            add_up(lax.rem(last + j, per), sub)
    for sub in range(lanes):
        finish(DOWN, sub)
        block(k, owners[hops], sub)
    for sub in range(lanes):
        add_up(last, sub)

    turned = jnp.transpose(stat[...])
    stat_out[...] = jnp.broadcast_to(jnp.sum(turned, axis=0, keepdims=True), stat_out.shape)
    stats = []
    for d in range(1, tp):
        copy = pltpu.make_async_remote_copy(
            src_ref=stat_out,
            dst_ref=stat_in.at[d],
            send_sem=st_send.at[d],
            recv_sem=st_recv.at[d],
            device_id={"fs": me_fs, "tp": lax.rem(me + d, tp)},
            device_id_type=MESH,
        )
        copy.start()
        stats.append(copy)
    for copy in started:
        copy.wait_send()
    for copy in inners:
        copy.wait_send()
    if cores > 1:
        swap.wait_send()
    for d, copy in sums:
        @pl.when(d != 0)
        def _(copy=copy):
            copy.wait_send()
    for copy in stats:
        copy.wait()
    squares = stat_out[...]
    for d in range(1, tp):
        squares = squares + stat_in[d]
    factor = lax.rsqrt(squares / width + EPS)
    stat[...] = jnp.transpose(jnp.broadcast_to(factor[0:1], (128, seq)))

    @pl.loop(0, seq // 128)
    def _(i):
        r = pl.ds(pl.multiple_of(i * 128, 128), 128)
        out_ref[r, :] = (total[r, :] * stat[r, 0:1] * gout_ref[...]).astype(jnp.bfloat16)


def ring_local(order, tokens, pool_weight, pool_scale, gain_mix, gain_mlp, w_up, w_down, gain_out):
    n, tp = lax.axis_size("fs"), lax.axis_size("tp")
    rows, width = tokens.shape
    hid, cols = w_up.shape
    seq, own = rows * tp, width // tp
    bf, f32 = jnp.bfloat16, jnp.float32
    vmem = pl.BlockSpec(memory_space=pltpu.VMEM)
    dma = pltpu.SemaphoreType.DMA
    lanes = 2 if cols % 256 == 0 else 1
    return pl.pallas_call(
        functools.partial(ring_kernel, n, tp, order),
        out_shape=jax.ShapeDtypeStruct((seq, own), bf),
        in_specs=[vmem] * 8,
        out_specs=vmem,
        scratch_shapes=[
            pltpu.VMEM((pool_weight.shape[0], pool_weight.shape[1] * n, pool_weight.shape[2]), bf),
            pltpu.VMEM((hid, width), bf),
            pltpu.VMEM((hid, width), bf),
            pltpu.VMEM((rows + 2 * HALO, width), f32),
            pltpu.VMEM((rows, width), bf),
            pltpu.VMEM((seq, width), bf),
            pltpu.VMEM((seq, hid), bf),
            pltpu.VMEM((seq, own), bf),
            pltpu.VMEM((n, lanes, seq, cols // lanes), bf),
            pltpu.VMEM((tp, n // tp, lanes, seq, cols // lanes), bf),
            pltpu.VMEM((HALO, width), bf),
            pltpu.VMEM((HALO, width), bf),
            pltpu.VMEM((2, HALO, width), bf),
            pltpu.VMEM((seq, own), f32),
            pltpu.VMEM((seq, 128), f32),
            pltpu.VMEM((8, seq), f32),
            pltpu.VMEM((tp, 8, seq), f32),
            dma((12 * (n // 2) + 2 * lanes,)),
            dma((12 * (n // 2) + 2 * lanes,)),
            dma((tp,)),
            dma((tp,)),
            dma((tp,)),
            dma((tp,)),
            dma((2,)),
            dma((2,)),
            dma((n * lanes,)),
            dma((n * lanes,)),
            dma,
            dma,
            dma((tp,)),
            dma((tp,)),
        ],
        compiler_params=pltpu.CompilerParams(
            collective_id=0, has_side_effects=True, vmem_limit_bytes=63 * 1024 * 1024
        ),
    )(
        tokens, pool_weight, w_up, w_down,
        pool_scale.reshape(1, -1), gain_mix.reshape(1, -1), gain_mlp.reshape(1, -1),
        gain_out.reshape(1, -1),
    )


NEAR = ((1, 2, 3), (0, 2, 3), (3, 1, 0), (2, 1, 0))
TARGETS = ((1, 2, 3), (0, 3, 2), (3, 0, 1), (2, 1, 0))
Y_FIRST = (True, False, True, False)
ENDS, INNER = 4, 4
UPS, DOWNS = 0, 1


def plane_kernel(
    tok_ref, pool_ref, up_ref, down_ref, scale_ref, gmix_ref, gmlp_ref, gout_ref, out_ref,
    pool_full, up_full, down_full, ext, first_all, inner, hidden,
    part_send, part_recv, part, y_recv, z_recv,
    before, after, edge, total, stat, stat_out, stat_in,
    pz_s, pz_r, px_s, px_r, swap_s, swap_r, wz_s, wz_r, wx_s, wx_r, halo_s, halo_r,
    f_s, f_r, d_s, d_r, y_s, y_r, z_s, z_r, st_s, st_r,
):
    rows, width = tok_ref.shape
    group = width // 4
    hid, cols = up_ref.shape
    depth = pool_ref.shape[1]
    nz, tp = 4, 4
    own_cols = width // tp
    seq = rows * tp
    most = max(ENDS, INNER)
    piece = hid // (ENDS + INNER)
    bf, f32 = jnp.bfloat16, jnp.float32
    me_fs, me = lax.axis_index("fs"), lax.axis_index("tp")
    z, x = lax.div(me_fs, 2), lax.rem(me_fs, 2)
    y, c = lax.div(me, 2), lax.rem(me, 2)
    q = lax.rem(z, 2)
    zp = z + 1 - 2 * q

    def pick(table, column):
        return lookup([row[column] for row in table], z)

    def is_end(plane):
        return (plane == 0) | (plane == nz - 1)

    def count_of(plane):
        return jnp.where(is_end(plane), ENDS, INNER)

    def base_of(plane):
        return jnp.where(is_end(plane), 0, ENDS * piece)

    def dev(z=z, x=x, y=y, c=c):
        return {"fs": z * 2 + x, "tp": y * 2 + c}

    def rc(src, dst, send, recv, to):
        return pltpu.make_async_remote_copy(
            src_ref=src, dst_ref=dst, send_sem=send, recv_sem=recv, device_id=to, device_id_type=MESH
        )

    def landed(dst, recv):
        pltpu.make_async_remote_copy(
            src_ref=dst, dst_ref=dst, send_sem=recv, recv_sem=recv, device_id=dev(x=1 - x), device_id_type=MESH
        ).wait_recv()

    barrier = pltpu.get_barrier_semaphore()
    peers = [dev(z=pick(TARGETS, k)) for k in range(3)] + [dev(x=1 - x), dev(y=1 - y), dev(c=1 - c)]
    peers.append(dev(y=1 - y, c=1 - c))
    for peer in peers:
        pl.semaphore_signal(barrier, inc=1, device_id=peer, device_id_type=MESH)
    pl.semaphore_wait(barrier, len(peers))

    always, pending = None, []

    def go(copy, condition=always):
        if condition is None:
            copy.start()
        else:
            @pl.when(condition)
            def _():
                copy.start()
        pending.append((copy, condition))

    gpc = pool_ref.shape[0] // 2
    mine_groups = pl.ds(c * gpc, gpc)

    def pool_block(plane, column):
        return pool_full.at[mine_groups, pl.ds(pl.multiple_of((plane * 2 + column) * depth, depth), depth), :]

    own_pool = pool_ref.at[mine_groups]
    for k in range(3):
        t = pick(TARGETS, k)
        go(rc(own_pool, pool_block(z, x), pz_s.at[t], pz_r.at[z], dev(z=t)))
    go(rc(own_pool, pool_block(z, x), px_s.at[z], px_r.at[z], dev(x=1 - x)))

    weights = (up_ref, down_ref)
    fulls = (up_full, down_full)

    def slot(stream, plane, p):
        return (stream * nz + plane) * most + p

    def block(stream, plane, column, p):
        return fulls[stream].at[
            pl.ds(p * piece, piece), pl.ds(pl.multiple_of((plane * 2 + column) * cols, cols), cols)
        ]

    def own_piece(stream, plane, p):
        start = pl.multiple_of(base_of(plane) + p * piece, piece)
        return weights[stream].at[pl.ds(start, piece), :]

    def some(p, plane):
        return always if p < min(ENDS, INNER) else p < count_of(plane)

    def spread_z(stream):
        for k in range(3):
            t = pick(TARGETS, k)
            for p in range(most):
                go(
                    rc(own_piece(stream, t, p), block(stream, z, x, p), wz_s.at[slot(stream, t, p)],
                       wz_r.at[slot(stream, z, p)], dev(z=t)),
                    some(p, t),
                )

    def spread_x(stream):
        for p in range(most):
            go(
                rc(own_piece(stream, z, p), block(stream, z, x, p), wx_s.at[slot(stream, z, p)],
                   wx_r.at[slot(stream, z, p)], dev(x=1 - x)),
                some(p, z),
            )

    def guarded(condition, body):
        if condition is None:
            body()
        else:
            pl.when(condition)(body)

    def relay(stream, k):
        s = pick(NEAR, k)
        for p in range(most):
            condition = some(p, z)
            ref = block(stream, s, x, p)
            guarded(condition, lambda ref=ref, p=p: landed(ref, wz_r.at[slot(stream, s, p)]))
            go(rc(ref, ref, wx_s.at[slot(stream, s, p)], wx_r.at[slot(stream, s, p)], dev(x=1 - x)), condition)

    def from_x(stream, s):
        for p in range(most):
            ref = block(stream, s, 1 - x, p)
            guarded(some(p, z), lambda ref=ref, p=p: landed(ref, wx_r.at[slot(stream, s, p)]))

    spread_z(UPS)
    spread_x(UPS)

    step = 32 if rows % 32 == 0 else rows

    @pl.loop(0, rows // step)
    def _(i):
        r = pl.ds(pl.multiple_of(i * step, step), step)
        v = tok_ref[r, :].astype(f32)
        v = v * lax.rsqrt(jnp.mean(v * v, axis=-1, keepdims=True) + EPS) * gmix_ref[...]
        v = v.astype(bf)
        ext[pl.ds(pl.multiple_of(HALO + i * step, HALO), step), :] = v.astype(f32)

    edge[0] = ext[rows : rows + HALO, :].astype(bf)
    edge[1] = ext[HALO : 2 * HALO, :].astype(bf)
    for side, (buffer, d) in enumerate(((before, 1), (after, tp - 1))):
        to = {"fs": me_fs, "tp": lax.rem(me + d, tp)}
        go(rc(edge.at[side], buffer, halo_s.at[side], halo_r.at[side], to))

    pool_full[mine_groups, pl.ds(pl.multiple_of(me_fs * depth, depth), depth), :] = pool_ref[mine_groups, :, :]
    for k in range(3):
        s = pick(NEAR, k)
        ref = pool_block(s, x)
        landed(ref, pz_r.at[s])
        go(rc(ref, ref, px_s.at[s], px_r.at[s], dev(x=1 - x)))
    mine = pl.ds(pl.multiple_of(me_fs * cols, cols), cols)
    for stream in (UPS, DOWNS):
        for p in range(most):
            def keep(stream=stream, p=p):
                start = pl.multiple_of(base_of(z) + p * piece, piece)
                fulls[stream][p * piece : (p + 1) * piece, mine] = weights[stream][pl.ds(start, piece), :]
            guarded(some(p, z), keep)
    landed(before, halo_r.at[0])
    landed(after, halo_r.at[1])
    offset = me * rows
    lower_open = (lax.rem(offset, SEQ_LEN) != 0).astype(f32)
    upper_open = (lax.rem(offset + rows, SEQ_LEN) != 0).astype(f32)
    ext[0:HALO, :] = before[...].astype(f32) * lower_open
    ext[rows + HALO : rows + 2 * HALO, :] = after[...].astype(f32) * upper_open
    for s in range(nz):
        landed(pool_block(s, 1 - x), px_r.at[s])
    go(rc(pool_full.at[mine_groups], pool_full.at[mine_groups], swap_s, swap_r, dev(c=1 - c)))
    landed(pool_full.at[pl.ds((1 - c) * gpc, gpc)], swap_r)

    def rows_of(s, t):
        return pl.ds(pl.multiple_of(s * seq + t * rows, rows), rows)

    my_rows = rows_of(q, me)
    position = lax.rem(offset + lax.broadcasted_iota(jnp.int32, (rows, 1), 0), SEQ_LEN)
    for index, reach in enumerate(WINDOWS):
        half = reach // 2
        g = slice(index * group, (index + 1) * group)
        level = ext[:, g]
        own = level[HALO : HALO + rows]
        shift = 1
        while shift < reach:
            level = level + pltpu.roll(level, shift, 0)
            shift *= 2
        if half > 1:
            level = pltpu.roll(level, rows + 2 * HALO - (half - 1), 0)
        window = level[HALO : HALO + rows]
        counts = (jnp.minimum(position + half, SEQ_LEN) - jnp.maximum(position - half, 0)).astype(f32)
        pooled = (window / counts - own).astype(bf)
        mixed = jnp.dot(pooled, pool_full[index], preferred_element_type=f32)
        first_all[my_rows, g] = (tok_ref[:, g].astype(f32) + mixed * scale_ref[:, g]).astype(bf)

    def share(s, t, k, to):
        ref = first_all.at[rows_of(s, t), :]
        go(rc(ref, ref, f_s.at[k], f_r.at[k], to))

    def shared(s, t, k):
        landed(first_all.at[rows_of(s, t), :], f_r.at[k])

    peer_y, peer_c = (1 - y) * 2 + c, y * 2 + 1 - c
    peer_yc = (1 - y) * 2 + 1 - c
    share(q, me, 0, dev(z=zp))
    share(q, me, 1, dev(y=1 - y))
    share(q, me, 3, dev(c=1 - c))
    spread_z(DOWNS)
    spread_x(DOWNS)
    for k in range(3):
        relay(UPS, k)

    def norm_up(s, yy):
        begin = s * seq + yy * 2 * rows

        @pl.loop(0, 2 * rows // step)
        def _(i):
            r = pl.ds(pl.multiple_of(begin + i * step, step), step)
            v = first_all[r, :].astype(f32)
            v = v * lax.rsqrt(jnp.mean(v * v, axis=-1, keepdims=True) + EPS) * gmlp_ref[...]
            inner[pl.ds(pl.multiple_of(i * step, step), step), :] = v.astype(bf)

        @pl.loop(0, count_of(z))
        def _(j):
            h = pl.ds(pl.multiple_of(j * piece, piece), piece)
            pre = lax.dot_general(
                inner[...], up_full[h, :], (((1,), (1,)), ((), ())), preferred_element_type=f32
            )
            hidden[pl.ds(pl.multiple_of(begin, 2 * rows), 2 * rows), h] = jnp.square(jnp.maximum(pre, 0.0)).astype(bf)

    shared(1 - q, me, 0)
    share(1 - q, me, 2, dev(y=1 - y))
    share(1 - q, me, 4, dev(c=1 - c))
    for s in range(nz):
        from_x(UPS, s)
    shared(q, peer_c, 3)
    norm_up(q, y)
    shared(q, peer_y, 1)
    share(q, peer_y, 5, dev(c=1 - c))
    shared(1 - q, peer_c, 4)
    norm_up(1 - q, y)
    relay(DOWNS, 0)
    shared(q, peer_yc, 5)
    norm_up(q, 1 - y)
    relay(DOWNS, 1)
    shared(1 - q, peer_y, 2)
    share(1 - q, peer_y, 6, dev(c=1 - c))
    shared(1 - q, peer_yc, 6)
    norm_up(1 - q, 1 - y)

    chunk = 2 * rows
    orow = pl.ds(pl.multiple_of(q * seq, seq), seq)
    prow = pl.ds(pl.multiple_of((1 - q) * seq, seq), seq)
    fine = 128

    def unit(i, j):
        plane = jnp.where(z < 2, i, nz - 1 - i)
        column = x if j == 0 else 1 - x
        return plane, column, (i // 2) * 2 + j, i * 2 + j

    def each(begin, size, body):
        @pl.loop(0, size // fine)
        def _(i):
            body(pl.ds(pl.multiple_of(begin + i * fine, fine), fine), pl.ds(pl.multiple_of(i * fine, fine), fine))

    def product(i, j):
        plane, column, s, u = unit(i, j)
        cc = pl.ds(pl.multiple_of((plane * 2 + column) * cols, cols), cols)
        theirs = lax.rem(plane, 2) != c
        if j == 1:
            from_x(DOWNS, plane)

        def all_rows(depth_of):
            @pl.loop(0, 2 * seq // chunk)
            def _(k):
                r = pl.ds(pl.multiple_of(k * chunk, chunk), chunk)
                value = jnp.dot(hidden[r, 0:depth_of], down_full[0:depth_of, cc], preferred_element_type=f32)

                @pl.when(theirs)
                def _():
                    part_send[s, r, :] = value.astype(bf)

                @pl.when(jnp.logical_not(theirs))
                def _():
                    part[s, r, :] = value

        if ENDS == INNER:
            all_rows(ENDS * piece)
        else:
            pl.when(is_end(z))(lambda: all_rows(ENDS * piece))
            pl.when(jnp.logical_not(is_end(z)))(lambda: all_rows(INNER * piece))
        go(rc(part_send.at[s], part_recv.at[s], d_s.at[u], d_r.at[u], dev(c=1 - c)), theirs)

    def stage1(i, j):
        plane, column, s, u = unit(i, j)
        ours = lax.rem(plane, 2) == c
        home = lax.div(plane, 2) == y

        def fold(begin, size, keep):
            def body(r, _):
                value = part[s, r, :] + part_recv[s, r, :].astype(f32)
                if keep:
                    part[s, r, :] = value
                else:
                    part_recv[s, r, :] = value.astype(bf)
            each(begin, size, body)

        @pl.when(ours)
        def _():
            landed(part_recv.at[s], d_r.at[u])
            if not Y_FIRST[i]:
                fold((1 - q) * seq, seq, False)

        if Y_FIRST[i]:
            pl.when(ours & home)(lambda: fold(0, 2 * seq, True))
            pl.when(ours & jnp.logical_not(home))(lambda: fold(0, 2 * seq, False))
            go(rc(part_recv.at[s], y_recv.at[j], y_s.at[u], y_r.at[u], dev(y=1 - y)), ours & jnp.logical_not(home))
        else:
            go(rc(part_recv.at[s, prow, :], z_recv.at[s], z_s.at[u], z_r.at[u], dev(z=zp)), ours)
            pl.when(ours)(lambda: fold(q * seq, seq, True))

    def stage2(i, j):
        plane, column, s, u = unit(i, j)
        ours = lax.rem(plane, 2) == c
        home = lax.div(plane, 2) == y
        if Y_FIRST[i]:
            @pl.when(ours & home)
            def _():
                landed(y_recv.at[j], y_r.at[u])

                def out(r, _):
                    y_recv[j, r, :] = (part[s, r, :] + y_recv[j, r, :].astype(f32)).astype(bf)
                each((1 - q) * seq, seq, out)

            go(rc(y_recv.at[j, prow, :], z_recv.at[s], z_s.at[u], z_r.at[u], dev(z=zp)), ours & home)

            @pl.when(ours & home)
            def _():
                def kept(r, _):
                    part[s, r, :] = part[s, r, :] + y_recv[j, r, :].astype(f32)
                each(q * seq, seq, kept)
        else:
            @pl.when(ours)
            def _():
                landed(z_recv.at[s], z_r.at[u])

            @pl.when(ours & jnp.logical_not(home))
            def _():
                def out(r, l):
                    part_recv[s, r, :] = (part[s, r, :] + z_recv[s, l, :].astype(f32)).astype(bf)
                each(q * seq, seq, out)

            go(rc(part_recv.at[s, orow, :], y_recv.at[j, orow, :], y_s.at[u], y_r.at[u], dev(y=1 - y)),
               ours & jnp.logical_not(home))

            @pl.when(ours & home)
            def _():
                def kept(r, l):
                    part[s, r, :] = part[s, r, :] + z_recv[s, l, :].astype(f32)
                each(q * seq, seq, kept)

    def stage3(i, j):
        plane, column, s, u = unit(i, j)

        @pl.when(plane == me)
        def _():
            if Y_FIRST[i]:
                landed(z_recv.at[s], z_r.at[u])
            else:
                landed(y_recv.at[j, orow, :], y_r.at[u])
            here = pl.ds(pl.multiple_of(column * cols, cols), cols)
            cc = pl.ds(pl.multiple_of(me * own_cols + column * cols, cols), cols)

            def body(r, l):
                more = z_recv[s, l, :] if Y_FIRST[i] else y_recv[j, r, :]
                value = part[s, r, :] + more.astype(f32) + first_all[r, cc].astype(f32)
                total[l, here] = value
                square = value * value
                lump = square[:, 0:128]
                for k in range(1, cols // 128):
                    lump = lump + square[:, k * 128 : (k + 1) * 128]
                stat[l, :] = stat[l, :] + lump
            each(q * seq, seq, body)

    stat[...] = jnp.zeros_like(stat)
    both = (0, 1)

    def run(body, i):
        for j in both:
            body(i, j)

    for i in range(3):
        run(product, i)
        run(stage1, i)
    for i in range(3):
        run(stage2, i)
    relay(DOWNS, 2)
    run(product, 3)
    run(stage1, 3)
    run(stage3, 0)
    run(stage3, 1)
    run(stage2, 3)
    run(stage3, 2)
    run(stage3, 3)

    turned = jnp.transpose(stat[...])
    stat_out[...] = jnp.broadcast_to(jnp.sum(turned, axis=0, keepdims=True), stat_out.shape)
    for d in range(1, tp):
        to = {"fs": me_fs, "tp": lax.rem(me + d, tp)}
        go(rc(stat_out, stat_in.at[d], st_s.at[d], st_r.at[d], to))
    for copy, condition in pending:
        guarded(condition, copy.wait_send)
    squares = stat_out[...]
    for d in range(1, tp):
        landed(stat_in.at[d], st_r.at[d])
        squares = squares + stat_in[d]
    factor = lax.rsqrt(squares / width + EPS)
    stat[...] = jnp.transpose(jnp.broadcast_to(factor[0:1], (128, seq)))

    @pl.loop(0, seq // 128)
    def _(i):
        r = pl.ds(pl.multiple_of(i * 128, 128), 128)
        out_ref[r, :] = (total[r, :] * stat[r, 0:1] * gout_ref[...]).astype(bf)


def plane_local(tokens, pool_weight, pool_scale, gain_mix, gain_mlp, w_up, w_down, gain_out):
    n, tp = lax.axis_size("fs"), lax.axis_size("tp")
    rows, width = tokens.shape
    hid, cols = w_up.shape
    seq, own = rows * tp, width // tp
    bf, f32 = jnp.bfloat16, jnp.float32
    vmem = pl.BlockSpec(memory_space=pltpu.VMEM)
    dma = pltpu.SemaphoreType.DMA
    most = max(ENDS, INNER)
    deep = hid // (ENDS + INNER) * most
    lots = 2 * 4 * most
    return pl.pallas_call(
        plane_kernel,
        out_shape=jax.ShapeDtypeStruct((seq, own), bf),
        in_specs=[vmem] * 8,
        out_specs=vmem,
        scratch_shapes=[
            pltpu.VMEM((pool_weight.shape[0], pool_weight.shape[1] * n, pool_weight.shape[2]), bf),
            pltpu.VMEM((deep, width), bf),
            pltpu.VMEM((deep, width), bf),
            pltpu.VMEM((rows + 2 * HALO, width), f32),
            pltpu.VMEM((2 * seq, width), bf),
            pltpu.VMEM((2 * rows, width), bf),
            pltpu.VMEM((2 * seq, deep), bf),
            pltpu.VMEM((4, 2 * seq, cols), bf),
            pltpu.VMEM((4, 2 * seq, cols), bf),
            pltpu.VMEM((4, 2 * seq, cols), f32),
            pltpu.VMEM((2, 2 * seq, cols), bf),
            pltpu.VMEM((4, seq, cols), bf),
            pltpu.VMEM((HALO, width), bf),
            pltpu.VMEM((HALO, width), bf),
            pltpu.VMEM((2, HALO, width), bf),
            pltpu.VMEM((seq, own), f32),
            pltpu.VMEM((seq, 128), f32),
            pltpu.VMEM((8, seq), f32),
            pltpu.VMEM((tp, 8, seq), f32),
            dma((4,)), dma((4,)), dma((4,)), dma((4,)), dma, dma,
            dma((lots,)), dma((lots,)), dma((lots,)), dma((lots,)),
            dma((2,)), dma((2,)),
            dma((7,)), dma((7,)),
            dma((8,)), dma((8,)), dma((8,)), dma((8,)), dma((8,)), dma((8,)),
            dma((tp,)), dma((tp,)),
        ],
        compiler_params=pltpu.CompilerParams(
            collective_id=0, has_side_effects=True, vmem_limit_bytes=63 * 1024 * 1024
        ),
    )(
        tokens, pool_weight, w_up, w_down,
        pool_scale.reshape(1, -1), gain_mix.reshape(1, -1), gain_mlp.reshape(1, -1),
        gain_out.reshape(1, -1),
    )


def grid_width(mesh):
    n = mesh.shape["fs"]
    try:
        line = mesh.devices.reshape(n, -1)[:, 0]
        nx = len({d.coords[0] for d in line})
        if n % nx == 0:
            return nx
    except AttributeError:
        pass
    return 2 if n % 2 == 0 else 1


def solution(mesh):
    n, tp, nx = mesh.shape["fs"], mesh.shape["tp"], grid_width(mesh)
    if nx == 2 and n == 8 and tp == 4:
        body = plane_local
    else:
        body = functools.partial(ring_local, ring_order(n, nx))
    return jax.shard_map(
        body,
        mesh=mesh,
        in_specs=(
            P(("fs", "tp"), None),
            P(None, "fs", None),
            P(),
            P(),
            P(),
            P("tp", "fs"),
            P("tp", "fs"),
            P("tp"),
        ),
        out_specs=P("fs", "tp"),
        check_vma=False,
    )
```

```python
import functools

import jax
import jax.numpy as jnp
from jax import lax
from jax.experimental import pallas as pl
from jax.experimental.pallas import tpu as pltpu
from jax.sharding import PartitionSpec as P

SEQ_LEN = 1024
EPS = 1e-06
WINDOWS = (2, 4, 8, 16)
HALO = 16
MESH = pl.DeviceIdType.MESH
POOL, UP, DOWN = 0, 1, 2


def ring_order(n, nx):
    nz = n // nx
    if nx < 2 or nz < 2 or nz % 2:
        return list(range(n))
    order = []
    for z in range(nz):
        xs = list(range(1, nx))
        order += [z * nx + x for x in (xs if z % 2 == 0 else xs[::-1])]
    return order + [z * nx for z in range(nz - 1, -1, -1)]


def lookup(table, index):
    value = jnp.int32(table[0])
    for i in range(1, len(table)):
        value = jnp.where(index == i, jnp.int32(table[i]), value)
    return value


def ring_kernel(
    n, tp, order, tok_ref, pool_ref, up_ref, down_ref, scale_ref, gmix_ref, gmlp_ref,
    gout_ref, out_ref,
    pool_full, up_full, down_full, ext, first, inner_all, hidden, fcols, blocks, parts,
    before, after, edge, total, stat, stat_out, stat_in,
    ring_send, ring_recv, in_send, in_recv, fc_send, fc_recv, halo_send, halo_recv, rs_send, rs_recv,
    pair_send, pair_recv, st_send, st_recv,
):
    rows, width = tok_ref.shape
    group = width // 4
    hid, cols = up_ref.shape
    depth = pool_ref.shape[1]
    own_cols = width // tp
    per = n // tp
    seq = rows * tp
    me_fs, me = lax.axis_index("fs"), lax.axis_index("tp")
    place_of = [order.index(i) for i in range(n)]
    place = lookup(place_of, me_fs)

    def at(offset):
        return lookup(order, lax.rem(place + offset + 2 * n, n))

    owners = {0: me_fs}
    for d in range(1, n // 2 + 1):
        owners[d] = at(d)
        owners[-d] = at(-d)
    right, left = owners[1], owners[-1]

    barrier = pltpu.get_barrier_semaphore()
    for peer in (right, left):
        pl.semaphore_signal(barrier, inc=1, device_id={"fs": peer, "tp": me}, device_id_type=MESH)
    for d in range(1, tp):
        pl.semaphore_signal(
            barrier, inc=1, device_id={"fs": me_fs, "tp": lax.rem(me + d, tp)}, device_id_type=MESH
        )
    pl.semaphore_wait(barrier, 2 + tp - 1)

    hops = n // 2
    cores = 2 if tp % 2 == 0 else 1
    core = lax.rem(me, cores)
    lanes = 2 if cols % 256 == 0 else 1
    fine = cols // lanes

    def view(stream, full, owner, piece, sub=None):
        if stream == POOL:
            ref = pool_full if full else pool_ref
            half = ref.shape[0] // (2 * cores)
            r = pl.ds(pl.multiple_of(owner * depth, depth), depth) if full else slice(None)
            return ref.at[pl.ds((core * 2 + piece) * half, half), r, :]
        ref = (up_full if full else up_ref) if stream == UP else (down_full if full else down_ref)
        half = hid // 2
        c = pl.ds(pl.multiple_of(owner * cols, cols), cols) if full else slice(None)
        if sub is not None:
            c = pl.ds(pl.multiple_of(owner * cols + sub * fine, fine), fine)
        return ref.at[pl.ds(piece * half, half), c]

    def count(side, piece):
        return hops if piece == side else hops - 1

    def slot(stream, side, piece, hop, sub):
        if sub:
            return 12 * hops + side * (lanes - 1) + sub - 1
        return ((stream * 2 + side) * 2 + piece) * hops + hop

    def subs(stream, hop):
        return range(lanes) if stream == DOWN and hop == hops - 1 and hop > 0 else (None,)

    def ring(stream, side, piece, hop, sub):
        owner = owners[-hop] if side == 0 else owners[hop]
        return pltpu.make_async_remote_copy(
            src_ref=view(stream, hop > 0, owner, piece, sub),
            dst_ref=view(stream, True, owner, piece, sub),
            send_sem=ring_send.at[slot(stream, side, piece, hop, sub)],
            recv_sem=ring_recv.at[slot(stream, side, piece, hop, sub)],
            device_id={"fs": right if side == 0 else left, "tp": me},
            device_id_type=MESH,
        )

    started = []

    def arrived(stream, side, piece, hop, sub=None):
        owner = owners[-hop - 1] if side == 0 else owners[hop + 1]
        pltpu.make_async_remote_copy(
            src_ref=view(stream, True, owner, piece, sub),
            dst_ref=view(stream, True, owner, piece, sub),
            send_sem=ring_send.at[slot(stream, side, piece, hop, sub)],
            recv_sem=ring_recv.at[slot(stream, side, piece, hop, sub)],
            device_id={"fs": right if side == 0 else left, "tp": me},
            device_id_type=MESH,
        ).wait_recv()

    def start(stream, hop, which=(0, 1)):
        for w in which:
            for side in (0, 1):
                piece = side if w == 0 else 1 - side
                if hop < count(side, piece):
                    if hop > 0:
                        arrived(stream, side, piece, hop - 1)
                    for sub in subs(stream, hop):
                        copy = ring(stream, side, piece, hop, sub)
                        copy.start()
                        started.append(copy)

    def finish(stream, sub=None):
        for side in (0, 1):
            arrived(stream, side, side, hops - 1, sub)

    def settle(stream, hop):
        if hop == hops - 2:
            for side in (0, 1):
                arrived(stream, side, 1 - side, hop)

    start(POOL, 0)
    start(UP, 0, (0,))

    step = 32 if rows % 32 == 0 else rows

    @pl.loop(0, rows // step)
    def _(i):
        r = pl.ds(pl.multiple_of(i * step, step), step)
        x = tok_ref[r, :].astype(jnp.float32)
        y = x * lax.rsqrt(jnp.mean(x * x, axis=-1, keepdims=True) + EPS) * gmix_ref[...]
        y = y.astype(jnp.bfloat16)
        ext[pl.ds(pl.multiple_of(HALO + i * step, HALO), step), :] = y.astype(jnp.float32)

    edge[0] = ext[rows : rows + HALO, :].astype(jnp.bfloat16)
    edge[1] = ext[HALO : 2 * HALO, :].astype(jnp.bfloat16)
    halos = []
    for side, (buffer, d) in enumerate(((before, 1), (after, tp - 1))):
        copy = pltpu.make_async_remote_copy(
            src_ref=edge.at[side],
            dst_ref=buffer,
            send_sem=halo_send.at[side],
            recv_sem=halo_recv.at[side],
            device_id={"fs": me_fs, "tp": lax.rem(me + d, tp)},
            device_id_type=MESH,
        )
        copy.start()
        halos.append(copy)

    start(POOL, 1)
    start(UP, 0, (1,))
    for hop in range(2, hops):
        start(POOL, hop)
    share = pl.ds(core * (pool_full.shape[0] // cores), pool_full.shape[0] // cores)
    pool_full[share, pl.ds(pl.multiple_of(me_fs * depth, depth), depth), :] = pool_ref[share, :, :]
    mine = pl.ds(pl.multiple_of(me_fs * cols, cols), cols)
    up_full[:, mine] = up_ref[...]
    down_full[:, mine] = down_ref[...]
    for copy in halos:
        copy.wait()
    offset = me * rows
    lower_open = (lax.rem(offset, SEQ_LEN) != 0).astype(jnp.float32)
    upper_open = (lax.rem(offset + rows, SEQ_LEN) != 0).astype(jnp.float32)
    ext[0:HALO, :] = before[...].astype(jnp.float32) * lower_open
    ext[rows + HALO : rows + 2 * HALO, :] = after[...].astype(jnp.float32) * upper_open
    start(UP, 1)
    settle(POOL, hops - 2)
    finish(POOL)
    if cores > 1:
        swap = pltpu.make_async_remote_copy(
            src_ref=pool_full.at[share],
            dst_ref=pool_full.at[share],
            send_sem=pair_send,
            recv_sem=pair_recv,
            device_id={"fs": me_fs, "tp": me + 1 - 2 * core},
            device_id_type=MESH,
        )
        swap.start()
        other = pl.ds((1 - core) * (pool_full.shape[0] // cores), pool_full.shape[0] // cores)
        pltpu.make_async_remote_copy(
            src_ref=pool_full.at[other],
            dst_ref=pool_full.at[other],
            send_sem=pair_send,
            recv_sem=pair_recv,
            device_id={"fs": me_fs, "tp": me + 1 - 2 * core},
            device_id_type=MESH,
        ).wait_recv()

    position = lax.rem(offset + lax.broadcasted_iota(jnp.int32, (rows, 1), 0), SEQ_LEN)
    for index, reach in enumerate(WINDOWS):
        half = reach // 2
        c = slice(index * group, (index + 1) * group)
        level = ext[:, c]
        own = level[HALO : HALO + rows]
        shift = 1
        while shift < reach:
            level = level + pltpu.roll(level, shift, 0)
            shift *= 2
        if half > 1:
            level = pltpu.roll(level, rows + 2 * HALO - (half - 1), 0)
        window = level[HALO : HALO + rows]
        counts = (jnp.minimum(position + half, SEQ_LEN) - jnp.maximum(position - half, 0)).astype(jnp.float32)
        pooled = (window / counts - own).astype(jnp.bfloat16)
        mixed = jnp.dot(pooled, pool_full[index], preferred_element_type=jnp.float32)
        first[:, c] = (tok_ref[:, c].astype(jnp.float32) + mixed * scale_ref[:, c]).astype(jnp.bfloat16)
    for hop in range(2, 3):
        if hop < hops:
            start(UP, hop)

    @pl.loop(0, rows // step)
    def _(i):
        r = pl.ds(pl.multiple_of(i * step, step), step)
        x = first[r, :].astype(jnp.float32)
        y = x * lax.rsqrt(jnp.mean(x * x, axis=-1, keepdims=True) + EPS) * gmlp_ref[...]
        inner_all[pl.ds(pl.multiple_of(me * rows + i * step, step), step), :] = y.astype(jnp.bfloat16)

    my_rows = pl.ds(pl.multiple_of(me * rows, rows), rows)
    inners, firsts = [], []
    for d in range(1, tp):
        peer = lax.rem(me + d, tp)
        copy = pltpu.make_async_remote_copy(
            src_ref=inner_all.at[my_rows, :],
            dst_ref=inner_all.at[my_rows, :],
            send_sem=in_send.at[d],
            recv_sem=in_recv.at[d],
            device_id={"fs": me_fs, "tp": peer},
            device_id_type=MESH,
        )
        copy.start()
        inners.append(copy)
    for d in range(1, tp):
        peer = lax.rem(me + d, tp)
        copy = pltpu.make_async_remote_copy(
            src_ref=first.at[:, pl.ds(pl.multiple_of(peer * own_cols, own_cols), own_cols)],
            dst_ref=fcols.at[my_rows, :],
            send_sem=fc_send.at[d],
            recv_sem=fc_recv.at[d],
            device_id={"fs": me_fs, "tp": peer},
            device_id_type=MESH,
        )
        copy.start()
        firsts.append(copy)
    fcols[my_rows, :] = first[:, pl.ds(pl.multiple_of(me * own_cols, own_cols), own_cols)]

    for hop in range(3, hops):
        start(UP, hop)
    settle(UP, hops - 2)
    start(DOWN, 0)
    finish(UP)
    for d in range(1, tp):
        source = pl.ds(pl.multiple_of(lax.rem(me + tp - d, tp) * rows, rows), rows)
        pltpu.make_async_remote_copy(
            src_ref=inner_all.at[source, :],
            dst_ref=inner_all.at[source, :],
            send_sem=in_send.at[d],
            recv_sem=in_recv.at[d],
            device_id={"fs": me_fs, "tp": lax.rem(me + d, tp)},
            device_id_type=MESH,
        ).wait_recv()

    tile = min(256, hid)

    @pl.loop(0, hid // tile)
    def _(j):
        h = pl.ds(pl.multiple_of(j * tile, tile), tile)
        pre = lax.dot_general(
            inner_all[...], up_full[h, :], (((1,), (1,)), ((), ())), preferred_element_type=jnp.float32
        )
        hidden[:, h] = jnp.square(jnp.maximum(pre, 0.0)).astype(jnp.bfloat16)

    sums = []
    part = min(512, seq)

    def block(k, owner, sub):
        c = pl.ds(pl.multiple_of(owner * cols + sub * fine, fine), fine)

        @pl.loop(0, seq // part)
        def _(i):
            r = pl.ds(pl.multiple_of(i * part, part), part)
            blocks[k, sub, r, :] = jnp.dot(
                hidden[r, :], down_full[:, c], preferred_element_type=jnp.float32
            ).astype(jnp.bfloat16)

        dest = owner // per
        d = lax.rem(dest - me + tp, tp)
        local = lax.rem(owner, per)
        copy = pltpu.make_async_remote_copy(
            src_ref=blocks.at[k, sub],
            dst_ref=parts.at[d, local, sub],
            send_sem=rs_send.at[k * lanes + sub],
            recv_sem=rs_recv.at[(d * per + local) * lanes + sub],
            device_id={"fs": me_fs, "tp": dest},
            device_id_type=MESH,
        )

        @pl.when(d == 0)
        def _():
            parts[0, local, sub] = blocks[k, sub]

        @pl.when(d != 0)
        def _():
            copy.start()

        sums.append((d, copy))

    def add_up(local, sub):
        for d in range(1, tp):
            pltpu.make_async_remote_copy(
                src_ref=blocks.at[0, sub],
                dst_ref=parts.at[d, local, sub],
                send_sem=rs_send.at[0],
                recv_sem=rs_recv.at[(d * per + local) * lanes + sub],
                device_id={"fs": me_fs, "tp": lax.rem(me + d, tp)},
                device_id_type=MESH,
            ).wait_recv()
        c = pl.ds(pl.multiple_of(local * cols + sub * fine, fine), fine)

        @pl.loop(0, seq // 128)
        def _(i):
            r = pl.ds(pl.multiple_of(i * 128, 128), 128)
            value = parts[0, local, sub, r, :].astype(jnp.float32)
            for d in range(1, tp):
                value = value + parts[d, local, sub, r, :].astype(jnp.float32)
            value = value + fcols[r, c].astype(jnp.float32)
            total[r, c] = value
            square = value * value
            lump = square[:, 0:128]
            for j in range(1, fine // 128):
                lump = lump + square[:, j * 128 : (j + 1) * 128]
            stat[r, :] = stat[r, :] + lump

    for sub in range(lanes):
        block(0, owners[0], sub)
    stat[...] = jnp.zeros_like(stat)
    k = 1
    for hop in range(1, hops):
        start(DOWN, hop)
        settle(DOWN, hop - 1)
        for owner in (owners[-hop], owners[hop]):
            for sub in range(lanes):
                block(k, owner, sub)
            k += 1
    for copy in firsts:
        copy.wait()
    last = lax.rem(owners[hops], per)
    for j in range(1, per):
        for sub in range(lanes):
            add_up(lax.rem(last + j, per), sub)
    for sub in range(lanes):
        finish(DOWN, sub)
        block(k, owners[hops], sub)
    for sub in range(lanes):
        add_up(last, sub)

    turned = jnp.transpose(stat[...])
    stat_out[...] = jnp.broadcast_to(jnp.sum(turned, axis=0, keepdims=True), stat_out.shape)
    stats = []
    for d in range(1, tp):
        copy = pltpu.make_async_remote_copy(
            src_ref=stat_out,
            dst_ref=stat_in.at[d],
            send_sem=st_send.at[d],
            recv_sem=st_recv.at[d],
            device_id={"fs": me_fs, "tp": lax.rem(me + d, tp)},
            device_id_type=MESH,
        )
        copy.start()
        stats.append(copy)
    for copy in started:
        copy.wait_send()
    for copy in inners:
        copy.wait_send()
    if cores > 1:
        swap.wait_send()
    for d, copy in sums:
        @pl.when(d != 0)
        def _(copy=copy):
            copy.wait_send()
    for copy in stats:
        copy.wait()
    squares = stat_out[...]
    for d in range(1, tp):
        squares = squares + stat_in[d]
    factor = lax.rsqrt(squares / width + EPS)
    stat[...] = jnp.transpose(jnp.broadcast_to(factor[0:1], (128, seq)))

    @pl.loop(0, seq // 128)
    def _(i):
        r = pl.ds(pl.multiple_of(i * 128, 128), 128)
        out_ref[r, :] = (total[r, :] * stat[r, 0:1] * gout_ref[...]).astype(jnp.bfloat16)


def ring_local(order, tokens, pool_weight, pool_scale, gain_mix, gain_mlp, w_up, w_down, gain_out):
    n, tp = lax.axis_size("fs"), lax.axis_size("tp")
    rows, width = tokens.shape
    hid, cols = w_up.shape
    seq, own = rows * tp, width // tp
    bf, f32 = jnp.bfloat16, jnp.float32
    vmem = pl.BlockSpec(memory_space=pltpu.VMEM)
    dma = pltpu.SemaphoreType.DMA
    lanes = 2 if cols % 256 == 0 else 1
    return pl.pallas_call(
        functools.partial(ring_kernel, n, tp, order),
        out_shape=jax.ShapeDtypeStruct((seq, own), bf),
        in_specs=[vmem] * 8,
        out_specs=vmem,
        scratch_shapes=[
            pltpu.VMEM((pool_weight.shape[0], pool_weight.shape[1] * n, pool_weight.shape[2]), bf),
            pltpu.VMEM((hid, width), bf),
            pltpu.VMEM((hid, width), bf),
            pltpu.VMEM((rows + 2 * HALO, width), f32),
            pltpu.VMEM((rows, width), bf),
            pltpu.VMEM((seq, width), bf),
            pltpu.VMEM((seq, hid), bf),
            pltpu.VMEM((seq, own), bf),
            pltpu.VMEM((n, lanes, seq, cols // lanes), bf),
            pltpu.VMEM((tp, n // tp, lanes, seq, cols // lanes), bf),
            pltpu.VMEM((HALO, width), bf),
            pltpu.VMEM((HALO, width), bf),
            pltpu.VMEM((2, HALO, width), bf),
            pltpu.VMEM((seq, own), f32),
            pltpu.VMEM((seq, 128), f32),
            pltpu.VMEM((8, seq), f32),
            pltpu.VMEM((tp, 8, seq), f32),
            dma((12 * (n // 2) + 2 * lanes,)),
            dma((12 * (n // 2) + 2 * lanes,)),
            dma((tp,)),
            dma((tp,)),
            dma((tp,)),
            dma((tp,)),
            dma((2,)),
            dma((2,)),
            dma((n * lanes,)),
            dma((n * lanes,)),
            dma,
            dma,
            dma((tp,)),
            dma((tp,)),
        ],
        compiler_params=pltpu.CompilerParams(
            collective_id=0, has_side_effects=True, vmem_limit_bytes=63 * 1024 * 1024
        ),
    )(
        tokens, pool_weight, w_up, w_down,
        pool_scale.reshape(1, -1), gain_mix.reshape(1, -1), gain_mlp.reshape(1, -1),
        gain_out.reshape(1, -1),
    )


NEAR = ((1, 2, 3), (0, 2, 3), (3, 1, 0), (2, 1, 0))
TARGETS = ((1, 2, 3), (0, 3, 2), (3, 0, 1), (2, 1, 0))
Y_FIRST = (True, False, True, False)
ENDS, INNER = 4, 4
UPS, DOWNS = 0, 1
HALVES = 2


def plane_kernel(
    tok_ref, pool_ref, up_ref, down_ref, scale_ref, gmix_ref, gmlp_ref, gout_ref, out_ref,
    pool_full, up_full, down_full, ext, first_all, inner_all, hidden,
    part_send, part_recv, part, y_recv, z_recv,
    before, after, edge, total, stat, stat_out, stat_in,
    pz_s, pz_r, px_s, px_r, py_s, py_r, pc_s, pc_r, wz_s, wz_r, wx_s, wx_r, halo_s, halo_r,
    f_s, f_r, d_s, d_r, y_s, y_r, z_s, z_r, st_s, st_r,
):
    rows, width = tok_ref.shape
    group = width // 4
    hid, cols = up_ref.shape
    depth = pool_ref.shape[1]
    nz, tp = 4, 4
    own_cols = width // tp
    seq = rows * tp
    most = max(ENDS, INNER)
    piece = hid // (ENDS + INNER)
    bf, f32 = jnp.bfloat16, jnp.float32
    me_fs, me = lax.axis_index("fs"), lax.axis_index("tp")
    z, x = lax.div(me_fs, 2), lax.rem(me_fs, 2)
    y, c = lax.div(me, 2), lax.rem(me, 2)
    q = lax.rem(z, 2)
    zp = z + 1 - 2 * q

    def pick(table, column):
        return lookup([row[column] for row in table], z)

    def is_end(plane):
        return (plane == 0) | (plane == nz - 1)

    def count_of(plane):
        return jnp.where(is_end(plane), ENDS, INNER)

    def base_of(plane):
        return jnp.where(is_end(plane), 0, ENDS * piece)

    def dev(z=z, x=x, y=y, c=c):
        return {"fs": z * 2 + x, "tp": y * 2 + c}

    def rc(src, dst, send, recv, to):
        return pltpu.make_async_remote_copy(
            src_ref=src, dst_ref=dst, send_sem=send, recv_sem=recv, device_id=to, device_id_type=MESH
        )

    def landed(dst, recv):
        pltpu.make_async_remote_copy(
            src_ref=dst, dst_ref=dst, send_sem=recv, recv_sem=recv, device_id=dev(x=1 - x), device_id_type=MESH
        ).wait_recv()

    barrier = pltpu.get_barrier_semaphore()
    peers = [dev(z=pick(TARGETS, k)) for k in range(3)] + [dev(x=1 - x), dev(y=1 - y), dev(c=1 - c)]
    peers.append(dev(y=1 - y, c=1 - c))
    for peer in peers:
        pl.semaphore_signal(barrier, inc=1, device_id=peer, device_id_type=MESH)
    pl.semaphore_wait(barrier, len(peers))

    always, pending = None, []

    def go(copy, condition=always):
        if condition is None:
            copy.start()
        else:
            @pl.when(condition)
            def _():
                copy.start()
        pending.append((copy, condition))

    def pool_block(g, plane, column):
        return pool_full.at[g, pl.ds(pl.multiple_of((plane * 2 + column) * depth, depth), depth), :]

    def pool_to_y(ref, plane, column):
        f = plane * 2 + column
        go(rc(ref, pool_block(me, plane, column), py_s.at[f], py_r.at[f], dev(y=1 - y)))

    def pool_to_x(ref, plane):
        go(rc(ref, pool_block(me, plane, x), px_s.at[plane], px_r.at[plane], dev(x=1 - x)))

    def pool_to_c(g, k):
        go(rc(pool_full.at[g], pool_full.at[g], pc_s.at[k], pc_r.at[k], dev(c=1 - c)))

    own_pool = pool_ref.at[me]
    for k in range(3):
        t = pick(TARGETS, k)
        go(rc(own_pool, pool_block(me, z, x), pz_s.at[t], pz_r.at[z], dev(z=t)))
    pool_to_x(own_pool, z)
    pool_to_y(own_pool, z, x)

    weights = (up_ref, down_ref)
    fulls = (up_full, down_full)

    def slot(stream, plane, p):
        return (stream * nz + plane) * most + p

    def block(stream, plane, column, p):
        return fulls[stream].at[
            pl.ds(p * piece, piece), pl.ds(pl.multiple_of((plane * 2 + column) * cols, cols), cols)
        ]

    def own_piece(stream, plane, p):
        start = pl.multiple_of(base_of(plane) + p * piece, piece)
        return weights[stream].at[pl.ds(start, piece), :]

    def some(p, plane):
        return always if p < min(ENDS, INNER) else p < count_of(plane)

    def spread_z(stream, order):
        for p, k in order:
            t = pick(TARGETS, k)
            go(
                rc(own_piece(stream, t, p), block(stream, z, x, p), wz_s.at[slot(stream, t, p)],
                   wz_r.at[slot(stream, z, p)], dev(z=t)),
                some(p, t),
            )

    def spread_x(stream, pieces):
        for p in pieces:
            go(
                rc(own_piece(stream, z, p), block(stream, z, x, p), wx_s.at[slot(stream, z, p)],
                   wx_r.at[slot(stream, z, p)], dev(x=1 - x)),
                some(p, z),
            )

    def guarded(condition, body):
        if condition is None:
            body()
        else:
            pl.when(condition)(body)

    def relay(stream, k, pieces):
        s = pick(NEAR, k)
        for p in pieces:
            condition = some(p, z)
            ref = block(stream, s, x, p)
            guarded(condition, lambda ref=ref, p=p: landed(ref, wz_r.at[slot(stream, s, p)]))
            go(rc(ref, ref, wx_s.at[slot(stream, s, p)], wx_r.at[slot(stream, s, p)], dev(x=1 - x)), condition)

    def from_x(stream, s, pieces):
        for p in pieces:
            ref = block(stream, s, 1 - x, p)
            guarded(some(p, z), lambda ref=ref, p=p: landed(ref, wx_r.at[slot(stream, s, p)]))

    every = range(most)
    early = range(most // 2)
    late = range(most // 2, most)
    spread_z(UPS, [(p, k) for p in every for k in range(3)])
    spread_x(UPS, early)

    step = 32 if rows % 32 == 0 else rows

    @pl.loop(0, rows // step)
    def _(i):
        r = pl.ds(pl.multiple_of(i * step, step), step)
        v = tok_ref[r, :].astype(f32)
        v = v * lax.rsqrt(jnp.mean(v * v, axis=-1, keepdims=True) + EPS) * gmix_ref[...]
        v = v.astype(bf)
        ext[pl.ds(pl.multiple_of(HALO + i * step, HALO), step), :] = v.astype(f32)

    edge[0] = ext[rows : rows + HALO, :].astype(bf)
    edge[1] = ext[HALO : 2 * HALO, :].astype(bf)
    for side, (buffer, d) in enumerate(((before, 1), (after, tp - 1))):
        to = {"fs": me_fs, "tp": lax.rem(me + d, tp)}
        go(rc(edge.at[side], buffer, halo_s.at[side], halo_r.at[side], to))

    pool_full[me, pl.ds(pl.multiple_of(me_fs * depth, depth), depth), :] = pool_ref[me, :, :]
    for k in range(3):
        s = pick(NEAR, k)
        ref = pool_block(me, s, x)
        landed(ref, pz_r.at[s])
        pool_to_x(ref, s)
        pool_to_y(ref, s, x)
    spread_x(UPS, late)
    mine = pl.ds(pl.multiple_of(me_fs * cols, cols), cols)
    for stream in (UPS, DOWNS):
        for p in range(most):
            def keep(stream=stream, p=p):
                start = pl.multiple_of(base_of(z) + p * piece, piece)
                fulls[stream][p * piece : (p + 1) * piece, mine] = weights[stream][pl.ds(start, piece), :]
            guarded(some(p, z), keep)
    landed(before, halo_r.at[0])
    landed(after, halo_r.at[1])
    offset = me * rows
    lower_open = (lax.rem(offset, SEQ_LEN) != 0).astype(f32)
    upper_open = (lax.rem(offset + rows, SEQ_LEN) != 0).astype(f32)
    ext[0:HALO, :] = before[...].astype(f32) * lower_open
    ext[rows + HALO : rows + 2 * HALO, :] = after[...].astype(f32) * upper_open
    for k in range(nz):
        s = z if k == 0 else pick(NEAR, k - 1)
        ref = pool_block(me, s, 1 - x)
        landed(ref, px_r.at[s])
        pool_to_y(ref, s, 1 - x)
    pool_to_c(me, 0)
    peer_c, peer_y, peer_yc = y * 2 + 1 - c, (1 - y) * 2 + c, (1 - y) * 2 + 1 - c
    for f in range(2 * nz):
        landed(pool_block(peer_y, f // 2, f % 2), py_r.at[f])
    pool_to_c(peer_y, 1)
    landed(pool_full.at[peer_c], pc_r.at[0])
    landed(pool_full.at[peer_yc], pc_r.at[1])

    def rows_of(s, t):
        return pl.ds(pl.multiple_of(s * seq + t * rows, rows), rows)

    my_rows = rows_of(q, me)
    position = lax.rem(offset + lax.broadcasted_iota(jnp.int32, (rows, 1), 0), SEQ_LEN)
    for index, reach in enumerate(WINDOWS):
        half = reach // 2
        g = slice(index * group, (index + 1) * group)
        level = ext[:, g]
        own = level[HALO : HALO + rows]
        shift = 1
        while shift < reach:
            level = level + pltpu.roll(level, shift, 0)
            shift *= 2
        if half > 1:
            level = pltpu.roll(level, rows + 2 * HALO - (half - 1), 0)
        window = level[HALO : HALO + rows]
        counts = (jnp.minimum(position + half, SEQ_LEN) - jnp.maximum(position - half, 0)).astype(f32)
        pooled = (window / counts - own).astype(bf)
        mixed = jnp.dot(pooled, pool_full[index], preferred_element_type=f32)
        first_all[my_rows, g] = (tok_ref[:, g].astype(f32) + mixed * scale_ref[:, g]).astype(bf)

    part_rows = rows // HALVES

    def first_part(s, t, h):
        return first_all.at[pl.ds(pl.multiple_of(s * seq + t * rows + h * part_rows, part_rows), part_rows), :]

    def share(s, t, k, to, h):
        ref = first_part(s, t, h)
        go(rc(ref, ref, f_s.at[k * HALVES + h], f_r.at[k * HALVES + h], to))

    def shared(s, t, k, h):
        landed(first_part(s, t, h), f_r.at[k * HALVES + h])

    halves = range(HALVES)
    for h in halves:
        share(q, me, 0, dev(z=zp), h)
        share(q, me, 1, dev(y=1 - y), h)
        share(q, me, 3, dev(c=1 - c), h)

    def groups(s, yy):
        return s * seq + yy * 2 * rows

    def norm(begin):
        @pl.loop(0, 2 * rows // step)
        def _(i):
            r = pl.ds(pl.multiple_of(begin + i * step, step), step)
            v = first_all[r, :].astype(f32)
            v = v * lax.rsqrt(jnp.mean(v * v, axis=-1, keepdims=True) + EPS) * gmlp_ref[...]
            inner_all[r, :] = v.astype(bf)

    def up(begin, lo, hi):
        g = pl.ds(pl.multiple_of(begin, 2 * rows), 2 * rows)

        @pl.loop(lo, hi)
        def _(j):
            h = pl.ds(pl.multiple_of(j * piece, piece), piece)
            pre = lax.dot_general(
                inner_all[g, :], up_full[h, :], (((1,), (1,)), ((), ())), preferred_element_type=f32
            )
            hidden[g, h] = jnp.square(jnp.maximum(pre, 0.0)).astype(bf)

    def pull(pieces):
        for p in pieces:
            for k in range(3):
                relay(UPS, k, (p,))

    def ready(pieces):
        for s in range(nz):
            from_x(UPS, s, pieces)

    def forward_z():
        for h in halves:
            shared(1 - q, me, 0, h)
            share(1 - q, me, 2, dev(y=1 - y), h)
            share(1 - q, me, 4, dev(c=1 - c), h)

    def forward_y(s, k, kc):
        for h in halves:
            shared(s, peer_y, k, h)
            share(s, peer_y, kc, dev(c=1 - c), h)

    def from_c(s, t, k):
        for h in halves:
            shared(s, t, k, h)

    g0, g1, g2, g3 = groups(q, y), groups(q, 1 - y), groups(1 - q, y), groups(1 - q, 1 - y)
    quarter = most // 4
    p0, p1, p2, p3 = [range(k * quarter, most if k == 3 else (k + 1) * quarter) for k in range(4)]
    half = 2 * quarter
    pull(p0)
    from_c(q, peer_c, 3)
    norm(g0)
    pull(p1)
    ready(p0)
    ready(p1)
    up(g0, 0, half)
    spread_x(DOWNS, every)
    forward_y(q, 1, 5)
    from_c(q, peer_yc, 5)
    norm(g1)
    up(g1, 0, half)
    pull(p2)
    forward_z()
    spread_z(DOWNS, [(p, k) for k in range(3) for p in every])
    pull(p3)
    from_c(1 - q, peer_c, 4)
    norm(g2)
    up(g2, 0, half)
    ready(p2)
    ready(p3)
    up(g0, half, count_of(z))
    up(g1, half, count_of(z))
    up(g2, half, count_of(z))
    relay(DOWNS, 0, every)
    forward_y(1 - q, 2, 6)
    from_c(1 - q, peer_yc, 6)
    norm(g3)
    up(g3, 0, count_of(z))
    first_sends = list(pending)
    pending.clear()

    chunk = 2 * rows
    orow = pl.ds(pl.multiple_of(q * seq, seq), seq)
    prow = pl.ds(pl.multiple_of((1 - q) * seq, seq), seq)
    fine = 128

    def unit(i, j):
        plane = jnp.where(z < 2, i, nz - 1 - i)
        column = x if j == 0 else 1 - x
        return plane, column, (i // 2) * 2 + j, i * 2 + j

    def each(begin, size, body):
        @pl.loop(0, size // fine)
        def _(i):
            body(pl.ds(pl.multiple_of(begin + i * fine, fine), fine), pl.ds(pl.multiple_of(i * fine, fine), fine))

    def send_part(i, j):
        plane, column, s, u = unit(i, j)
        go(rc(part_send.at[s], part_recv.at[s], d_s.at[u], d_r.at[u], dev(c=1 - c)), lax.rem(plane, 2) != c)

    def multiply(theirs, deep, cc, slots):
        def all_rows(theirs, deep):
            @pl.loop(0, 2 * seq // chunk)
            def _(k):
                r = pl.ds(pl.multiple_of(k * chunk, chunk), chunk)
                value = jnp.dot(hidden[r, 0:deep], down_full[0:deep, cc], preferred_element_type=f32)
                for n, s in enumerate(slots):
                    lane = slice(n * cols, (n + 1) * cols)
                    if theirs:
                        part_send[s, r, :] = value[:, lane].astype(bf)
                    else:
                        part[s, r, :] = value[:, lane]

        pl.when(theirs)(lambda: all_rows(True, deep))
        pl.when(jnp.logical_not(theirs))(lambda: all_rows(False, deep))

    def by_depth(body):
        if ENDS == INNER:
            body(ENDS * piece)
        else:
            pl.when(is_end(z))(lambda: body(ENDS * piece))
            pl.when(jnp.logical_not(is_end(z)))(lambda: body(INNER * piece))

    def product(i, j):
        plane, column, s, u = unit(i, j)
        cc = pl.ds(pl.multiple_of((plane * 2 + column) * cols, cols), cols)
        if j == 1:
            from_x(DOWNS, plane, every)
        by_depth(lambda deep: multiply(lax.rem(plane, 2) != c, deep, cc, (s,)))
        send_part(i, j)

    def wide_product(i):
        plane = jnp.where(z < 2, i, nz - 1 - i)
        cc = pl.ds(pl.multiple_of(plane * 2 * cols, 2 * cols), 2 * cols)
        from_x(DOWNS, plane, every)
        slots = ((i // 2) * 2 + x, (i // 2) * 2 + 1 - x)
        by_depth(lambda deep: multiply(lax.rem(plane, 2) != c, deep, cc, slots))
        for j in (0, 1):
            send_part(i, j)

    def stage1(i, j):
        plane, column, s, u = unit(i, j)
        ours = lax.rem(plane, 2) == c
        home = lax.div(plane, 2) == y

        def fold(begin, size, keep):
            def body(r, _):
                value = part[s, r, :] + part_recv[s, r, :].astype(f32)
                if keep:
                    part[s, r, :] = value
                else:
                    part_recv[s, r, :] = value.astype(bf)
            each(begin, size, body)

        @pl.when(ours)
        def _():
            landed(part_recv.at[s], d_r.at[u])
            if not Y_FIRST[i]:
                fold((1 - q) * seq, seq, False)

        if Y_FIRST[i]:
            pl.when(ours & home)(lambda: fold(0, 2 * seq, True))
            pl.when(ours & jnp.logical_not(home))(lambda: fold(0, 2 * seq, False))
            go(rc(part_recv.at[s], y_recv.at[j], y_s.at[u], y_r.at[u], dev(y=1 - y)), ours & jnp.logical_not(home))
        else:
            go(rc(part_recv.at[s, prow, :], z_recv.at[s], z_s.at[u], z_r.at[u], dev(z=zp)), ours)
            pl.when(ours)(lambda: fold(q * seq, seq, True))

    def stage2(i, j):
        plane, column, s, u = unit(i, j)
        ours = lax.rem(plane, 2) == c
        home = lax.div(plane, 2) == y
        if Y_FIRST[i]:
            @pl.when(ours & home)
            def _():
                landed(y_recv.at[j], y_r.at[u])

                def out(r, _):
                    y_recv[j, r, :] = (part[s, r, :] + y_recv[j, r, :].astype(f32)).astype(bf)
                each((1 - q) * seq, seq, out)

            go(rc(y_recv.at[j, prow, :], z_recv.at[s], z_s.at[u], z_r.at[u], dev(z=zp)), ours & home)

            @pl.when(ours & home)
            def _():
                def kept(r, _):
                    part[s, r, :] = part[s, r, :] + y_recv[j, r, :].astype(f32)
                each(q * seq, seq, kept)
        else:
            @pl.when(ours)
            def _():
                landed(z_recv.at[s], z_r.at[u])

            @pl.when(ours & jnp.logical_not(home))
            def _():
                def out(r, l):
                    part_recv[s, r, :] = (part[s, r, :] + z_recv[s, l, :].astype(f32)).astype(bf)
                each(q * seq, seq, out)

            go(rc(part_recv.at[s, orow, :], y_recv.at[j, orow, :], y_s.at[u], y_r.at[u], dev(y=1 - y)),
               ours & jnp.logical_not(home))

            @pl.when(ours & home)
            def _():
                def kept(r, l):
                    part[s, r, :] = part[s, r, :] + z_recv[s, l, :].astype(f32)
                each(q * seq, seq, kept)

    def stage3(i, j):
        plane, column, s, u = unit(i, j)

        @pl.when(plane == me)
        def _():
            if Y_FIRST[i]:
                landed(z_recv.at[s], z_r.at[u])
            else:
                landed(y_recv.at[j, orow, :], y_r.at[u])
            here = pl.ds(pl.multiple_of(column * cols, cols), cols)
            cc = pl.ds(pl.multiple_of(me * own_cols + column * cols, cols), cols)

            def body(r, l):
                more = z_recv[s, l, :] if Y_FIRST[i] else y_recv[j, r, :]
                value = part[s, r, :] + more.astype(f32) + first_all[r, cc].astype(f32)
                total[l, here] = value
                square = value * value
                lump = square[:, 0:128]
                for k in range(1, cols // 128):
                    lump = lump + square[:, k * 128 : (k + 1) * 128]
                stat[l, :] = stat[l, :] + lump
            each(q * seq, seq, body)

    stat[...] = jnp.zeros_like(stat)
    both = (0, 1)

    def run(body, i):
        for j in both:
            body(i, j)

    def drain():
        for copy, condition in pending:
            guarded(condition, copy.wait_send)
        pending.clear()

    wide_product(0)
    relay(DOWNS, 1, every)
    wide_product(1)
    run(stage1, 0)
    run(stage1, 1)
    wide_product(2)
    run(stage1, 2)
    relay(DOWNS, 2, every)
    run(product, 3)
    run(stage2, 1)
    run(stage1, 3)
    for copy, condition in first_sends:
        guarded(condition, copy.wait_send)
    run(stage2, 0)
    run(stage2, 2)
    run(stage2, 3)
    run(stage3, 0)
    run(stage3, 1)
    run(stage3, 2)
    run(stage3, 3)

    turned = jnp.transpose(stat[...])
    stat_out[...] = jnp.broadcast_to(jnp.sum(turned, axis=0, keepdims=True), stat_out.shape)
    for d in range(1, tp):
        to = {"fs": me_fs, "tp": lax.rem(me + d, tp)}
        go(rc(stat_out, stat_in.at[d], st_s.at[d], st_r.at[d], to))
    drain()
    squares = stat_out[...]
    for d in range(1, tp):
        landed(stat_in.at[d], st_r.at[d])
        squares = squares + stat_in[d]
    factor = lax.rsqrt(squares / width + EPS)
    stat[...] = jnp.transpose(jnp.broadcast_to(factor[0:1], (128, seq)))

    @pl.loop(0, seq // 128)
    def _(i):
        r = pl.ds(pl.multiple_of(i * 128, 128), 128)
        out_ref[r, :] = (total[r, :] * stat[r, 0:1] * gout_ref[...]).astype(bf)


def plane_local(tokens, pool_weight, pool_scale, gain_mix, gain_mlp, w_up, w_down, gain_out):
    n, tp = lax.axis_size("fs"), lax.axis_size("tp")
    rows, width = tokens.shape
    hid, cols = w_up.shape
    seq, own = rows * tp, width // tp
    bf, f32 = jnp.bfloat16, jnp.float32
    vmem = pl.BlockSpec(memory_space=pltpu.VMEM)
    dma = pltpu.SemaphoreType.DMA
    most = max(ENDS, INNER)
    deep = hid // (ENDS + INNER) * most
    lots = 2 * 4 * most
    return pl.pallas_call(
        plane_kernel,
        out_shape=jax.ShapeDtypeStruct((seq, own), bf),
        in_specs=[vmem] * 8,
        out_specs=vmem,
        scratch_shapes=[
            pltpu.VMEM((pool_weight.shape[0], pool_weight.shape[1] * n, pool_weight.shape[2]), bf),
            pltpu.VMEM((deep, width), bf),
            pltpu.VMEM((deep, width), bf),
            pltpu.VMEM((rows + 2 * HALO, width), f32),
            pltpu.VMEM((2 * seq, width), bf),
            pltpu.VMEM((2 * seq, width), bf),
            pltpu.VMEM((2 * seq, deep), bf),
            pltpu.VMEM((4, 2 * seq, cols), bf),
            pltpu.VMEM((4, 2 * seq, cols), bf),
            pltpu.VMEM((4, 2 * seq, cols), f32),
            pltpu.VMEM((2, 2 * seq, cols), bf),
            pltpu.VMEM((4, seq, cols), bf),
            pltpu.VMEM((HALO, width), bf),
            pltpu.VMEM((HALO, width), bf),
            pltpu.VMEM((2, HALO, width), bf),
            pltpu.VMEM((seq, own), f32),
            pltpu.VMEM((seq, 128), f32),
            pltpu.VMEM((8, seq), f32),
            pltpu.VMEM((tp, 8, seq), f32),
            dma((4,)), dma((4,)), dma((4,)), dma((4,)), dma((8,)), dma((8,)), dma((2,)), dma((2,)),
            dma((lots,)), dma((lots,)), dma((lots,)), dma((lots,)),
            dma((2,)), dma((2,)),
            dma((7 * HALVES,)), dma((7 * HALVES,)),
            dma((8,)), dma((8,)), dma((8,)), dma((8,)), dma((8,)), dma((8,)),
            dma((tp,)), dma((tp,)),
        ],
        compiler_params=pltpu.CompilerParams(
            collective_id=0, has_side_effects=True, vmem_limit_bytes=63 * 1024 * 1024
        ),
    )(
        tokens, pool_weight, w_up, w_down,
        pool_scale.reshape(1, -1), gain_mix.reshape(1, -1), gain_mlp.reshape(1, -1),
        gain_out.reshape(1, -1),
    )


def grid_width(mesh):
    n = mesh.shape["fs"]
    try:
        line = mesh.devices.reshape(n, -1)[:, 0]
        nx = len({d.coords[0] for d in line})
        if n % nx == 0:
            return nx
    except AttributeError:
        pass
    return 2 if n % 2 == 0 else 1


def solution(mesh):
    n, tp, nx = mesh.shape["fs"], mesh.shape["tp"], grid_width(mesh)
    if nx == 2 and n == 8 and tp == 4:
        body = plane_local
    else:
        body = functools.partial(ring_local, ring_order(n, nx))
    return jax.shard_map(
        body,
        mesh=mesh,
        in_specs=(
            P(("fs", "tp"), None),
            P(None, "fs", None),
            P(),
            P(),
            P(),
            P("tp", "fs"),
            P("tp", "fs"),
            P("tp"),
        ),
        out_specs=P("fs", "tp"),
        check_vma=False,
    )
```

```python
import functools

import jax
import jax.numpy as jnp
from jax import lax
from jax.experimental import pallas as pl
from jax.experimental.pallas import tpu as pltpu
from jax.sharding import PartitionSpec as P

SEQ_LEN = 1024
EPS = 1e-06
WINDOWS = (2, 4, 8, 16)
HALO = 16
MESH = pl.DeviceIdType.MESH
POOL, UP, DOWN = 0, 1, 2


def ring_order(n, nx):
    nz = n // nx
    if nx < 2 or nz < 2 or nz % 2:
        return list(range(n))
    order = []
    for z in range(nz):
        xs = list(range(1, nx))
        order += [z * nx + x for x in (xs if z % 2 == 0 else xs[::-1])]
    return order + [z * nx for z in range(nz - 1, -1, -1)]


def lookup(table, index):
    value = jnp.int32(table[0])
    for i in range(1, len(table)):
        value = jnp.where(index == i, jnp.int32(table[i]), value)
    return value


def ring_kernel(
    n, tp, order, tok_ref, pool_ref, up_ref, down_ref, scale_ref, gmix_ref, gmlp_ref,
    gout_ref, out_ref,
    pool_full, up_full, down_full, ext, first, inner_all, hidden, fcols, blocks, parts,
    before, after, edge, total, stat, stat_out, stat_in,
    ring_send, ring_recv, in_send, in_recv, fc_send, fc_recv, halo_send, halo_recv, rs_send, rs_recv,
    pair_send, pair_recv, st_send, st_recv,
):
    rows, width = tok_ref.shape
    group = width // 4
    hid, cols = up_ref.shape
    depth = pool_ref.shape[1]
    own_cols = width // tp
    per = n // tp
    seq = rows * tp
    me_fs, me = lax.axis_index("fs"), lax.axis_index("tp")
    place_of = [order.index(i) for i in range(n)]
    place = lookup(place_of, me_fs)

    def at(offset):
        return lookup(order, lax.rem(place + offset + 2 * n, n))

    owners = {0: me_fs}
    for d in range(1, n // 2 + 1):
        owners[d] = at(d)
        owners[-d] = at(-d)
    right, left = owners[1], owners[-1]

    barrier = pltpu.get_barrier_semaphore()
    for peer in (right, left):
        pl.semaphore_signal(barrier, inc=1, device_id={"fs": peer, "tp": me}, device_id_type=MESH)
    for d in range(1, tp):
        pl.semaphore_signal(
            barrier, inc=1, device_id={"fs": me_fs, "tp": lax.rem(me + d, tp)}, device_id_type=MESH
        )
    pl.semaphore_wait(barrier, 2 + tp - 1)

    hops = n // 2
    cores = 2 if tp % 2 == 0 else 1
    core = lax.rem(me, cores)
    lanes = 2 if cols % 256 == 0 else 1
    fine = cols // lanes

    def view(stream, full, owner, piece, sub=None):
        if stream == POOL:
            ref = pool_full if full else pool_ref
            half = ref.shape[0] // (2 * cores)
            r = pl.ds(pl.multiple_of(owner * depth, depth), depth) if full else slice(None)
            return ref.at[pl.ds((core * 2 + piece) * half, half), r, :]
        ref = (up_full if full else up_ref) if stream == UP else (down_full if full else down_ref)
        half = hid // 2
        c = pl.ds(pl.multiple_of(owner * cols, cols), cols) if full else slice(None)
        if sub is not None:
            c = pl.ds(pl.multiple_of(owner * cols + sub * fine, fine), fine)
        return ref.at[pl.ds(piece * half, half), c]

    def count(side, piece):
        return hops if piece == side else hops - 1

    def slot(stream, side, piece, hop, sub):
        if sub:
            return 12 * hops + side * (lanes - 1) + sub - 1
        return ((stream * 2 + side) * 2 + piece) * hops + hop

    def subs(stream, hop):
        return range(lanes) if stream == DOWN and hop == hops - 1 and hop > 0 else (None,)

    def ring(stream, side, piece, hop, sub):
        owner = owners[-hop] if side == 0 else owners[hop]
        return pltpu.make_async_remote_copy(
            src_ref=view(stream, hop > 0, owner, piece, sub),
            dst_ref=view(stream, True, owner, piece, sub),
            send_sem=ring_send.at[slot(stream, side, piece, hop, sub)],
            recv_sem=ring_recv.at[slot(stream, side, piece, hop, sub)],
            device_id={"fs": right if side == 0 else left, "tp": me},
            device_id_type=MESH,
        )

    started = []

    def arrived(stream, side, piece, hop, sub=None):
        owner = owners[-hop - 1] if side == 0 else owners[hop + 1]
        pltpu.make_async_remote_copy(
            src_ref=view(stream, True, owner, piece, sub),
            dst_ref=view(stream, True, owner, piece, sub),
            send_sem=ring_send.at[slot(stream, side, piece, hop, sub)],
            recv_sem=ring_recv.at[slot(stream, side, piece, hop, sub)],
            device_id={"fs": right if side == 0 else left, "tp": me},
            device_id_type=MESH,
        ).wait_recv()

    def start(stream, hop, which=(0, 1)):
        for w in which:
            for side in (0, 1):
                piece = side if w == 0 else 1 - side
                if hop < count(side, piece):
                    if hop > 0:
                        arrived(stream, side, piece, hop - 1)
                    for sub in subs(stream, hop):
                        copy = ring(stream, side, piece, hop, sub)
                        copy.start()
                        started.append(copy)

    def finish(stream, sub=None):
        for side in (0, 1):
            arrived(stream, side, side, hops - 1, sub)

    def settle(stream, hop):
        if hop == hops - 2:
            for side in (0, 1):
                arrived(stream, side, 1 - side, hop)

    start(POOL, 0)
    start(UP, 0, (0,))

    step = 32 if rows % 32 == 0 else rows

    @pl.loop(0, rows // step)
    def _(i):
        r = pl.ds(pl.multiple_of(i * step, step), step)
        x = tok_ref[r, :].astype(jnp.float32)
        y = x * lax.rsqrt(jnp.mean(x * x, axis=-1, keepdims=True) + EPS) * gmix_ref[...]
        y = y.astype(jnp.bfloat16)
        ext[pl.ds(pl.multiple_of(HALO + i * step, HALO), step), :] = y.astype(jnp.float32)

    edge[0] = ext[rows : rows + HALO, :].astype(jnp.bfloat16)
    edge[1] = ext[HALO : 2 * HALO, :].astype(jnp.bfloat16)
    halos = []
    for side, (buffer, d) in enumerate(((before, 1), (after, tp - 1))):
        copy = pltpu.make_async_remote_copy(
            src_ref=edge.at[side],
            dst_ref=buffer,
            send_sem=halo_send.at[side],
            recv_sem=halo_recv.at[side],
            device_id={"fs": me_fs, "tp": lax.rem(me + d, tp)},
            device_id_type=MESH,
        )
        copy.start()
        halos.append(copy)

    start(POOL, 1)
    start(UP, 0, (1,))
    for hop in range(2, hops):
        start(POOL, hop)
    share = pl.ds(core * (pool_full.shape[0] // cores), pool_full.shape[0] // cores)
    pool_full[share, pl.ds(pl.multiple_of(me_fs * depth, depth), depth), :] = pool_ref[share, :, :]
    mine = pl.ds(pl.multiple_of(me_fs * cols, cols), cols)
    up_full[:, mine] = up_ref[...]
    down_full[:, mine] = down_ref[...]
    for copy in halos:
        copy.wait()
    offset = me * rows
    lower_open = (lax.rem(offset, SEQ_LEN) != 0).astype(jnp.float32)
    upper_open = (lax.rem(offset + rows, SEQ_LEN) != 0).astype(jnp.float32)
    ext[0:HALO, :] = before[...].astype(jnp.float32) * lower_open
    ext[rows + HALO : rows + 2 * HALO, :] = after[...].astype(jnp.float32) * upper_open
    start(UP, 1)
    settle(POOL, hops - 2)
    finish(POOL)
    if cores > 1:
        swap = pltpu.make_async_remote_copy(
            src_ref=pool_full.at[share],
            dst_ref=pool_full.at[share],
            send_sem=pair_send,
            recv_sem=pair_recv,
            device_id={"fs": me_fs, "tp": me + 1 - 2 * core},
            device_id_type=MESH,
        )
        swap.start()
        other = pl.ds((1 - core) * (pool_full.shape[0] // cores), pool_full.shape[0] // cores)
        pltpu.make_async_remote_copy(
            src_ref=pool_full.at[other],
            dst_ref=pool_full.at[other],
            send_sem=pair_send,
            recv_sem=pair_recv,
            device_id={"fs": me_fs, "tp": me + 1 - 2 * core},
            device_id_type=MESH,
        ).wait_recv()

    position = lax.rem(offset + lax.broadcasted_iota(jnp.int32, (rows, 1), 0), SEQ_LEN)
    for index, reach in enumerate(WINDOWS):
        half = reach // 2
        c = slice(index * group, (index + 1) * group)
        level = ext[:, c]
        own = level[HALO : HALO + rows]
        shift = 1
        while shift < reach:
            level = level + pltpu.roll(level, shift, 0)
            shift *= 2
        if half > 1:
            level = pltpu.roll(level, rows + 2 * HALO - (half - 1), 0)
        window = level[HALO : HALO + rows]
        counts = (jnp.minimum(position + half, SEQ_LEN) - jnp.maximum(position - half, 0)).astype(jnp.float32)
        pooled = (window / counts - own).astype(jnp.bfloat16)
        mixed = jnp.dot(pooled, pool_full[index], preferred_element_type=jnp.float32)
        first[:, c] = (tok_ref[:, c].astype(jnp.float32) + mixed * scale_ref[:, c]).astype(jnp.bfloat16)
    for hop in range(2, 3):
        if hop < hops:
            start(UP, hop)

    @pl.loop(0, rows // step)
    def _(i):
        r = pl.ds(pl.multiple_of(i * step, step), step)
        x = first[r, :].astype(jnp.float32)
        y = x * lax.rsqrt(jnp.mean(x * x, axis=-1, keepdims=True) + EPS) * gmlp_ref[...]
        inner_all[pl.ds(pl.multiple_of(me * rows + i * step, step), step), :] = y.astype(jnp.bfloat16)

    my_rows = pl.ds(pl.multiple_of(me * rows, rows), rows)
    inners, firsts = [], []
    for d in range(1, tp):
        peer = lax.rem(me + d, tp)
        copy = pltpu.make_async_remote_copy(
            src_ref=inner_all.at[my_rows, :],
            dst_ref=inner_all.at[my_rows, :],
            send_sem=in_send.at[d],
            recv_sem=in_recv.at[d],
            device_id={"fs": me_fs, "tp": peer},
            device_id_type=MESH,
        )
        copy.start()
        inners.append(copy)
    for d in range(1, tp):
        peer = lax.rem(me + d, tp)
        copy = pltpu.make_async_remote_copy(
            src_ref=first.at[:, pl.ds(pl.multiple_of(peer * own_cols, own_cols), own_cols)],
            dst_ref=fcols.at[my_rows, :],
            send_sem=fc_send.at[d],
            recv_sem=fc_recv.at[d],
            device_id={"fs": me_fs, "tp": peer},
            device_id_type=MESH,
        )
        copy.start()
        firsts.append(copy)
    fcols[my_rows, :] = first[:, pl.ds(pl.multiple_of(me * own_cols, own_cols), own_cols)]

    for hop in range(3, hops):
        start(UP, hop)
    settle(UP, hops - 2)
    start(DOWN, 0)
    finish(UP)
    for d in range(1, tp):
        source = pl.ds(pl.multiple_of(lax.rem(me + tp - d, tp) * rows, rows), rows)
        pltpu.make_async_remote_copy(
            src_ref=inner_all.at[source, :],
            dst_ref=inner_all.at[source, :],
            send_sem=in_send.at[d],
            recv_sem=in_recv.at[d],
            device_id={"fs": me_fs, "tp": lax.rem(me + d, tp)},
            device_id_type=MESH,
        ).wait_recv()

    tile = min(256, hid)

    @pl.loop(0, hid // tile)
    def _(j):
        h = pl.ds(pl.multiple_of(j * tile, tile), tile)
        pre = lax.dot_general(
            inner_all[...], up_full[h, :], (((1,), (1,)), ((), ())), preferred_element_type=jnp.float32
        )
        hidden[:, h] = jnp.square(jnp.maximum(pre, 0.0)).astype(jnp.bfloat16)

    sums = []
    part = min(512, seq)

    def block(k, owner, sub):
        c = pl.ds(pl.multiple_of(owner * cols + sub * fine, fine), fine)

        @pl.loop(0, seq // part)
        def _(i):
            r = pl.ds(pl.multiple_of(i * part, part), part)
            blocks[k, sub, r, :] = jnp.dot(
                hidden[r, :], down_full[:, c], preferred_element_type=jnp.float32
            ).astype(jnp.bfloat16)

        dest = owner // per
        d = lax.rem(dest - me + tp, tp)
        local = lax.rem(owner, per)
        copy = pltpu.make_async_remote_copy(
            src_ref=blocks.at[k, sub],
            dst_ref=parts.at[d, local, sub],
            send_sem=rs_send.at[k * lanes + sub],
            recv_sem=rs_recv.at[(d * per + local) * lanes + sub],
            device_id={"fs": me_fs, "tp": dest},
            device_id_type=MESH,
        )

        @pl.when(d == 0)
        def _():
            parts[0, local, sub] = blocks[k, sub]

        @pl.when(d != 0)
        def _():
            copy.start()

        sums.append((d, copy))

    def add_up(local, sub):
        for d in range(1, tp):
            pltpu.make_async_remote_copy(
                src_ref=blocks.at[0, sub],
                dst_ref=parts.at[d, local, sub],
                send_sem=rs_send.at[0],
                recv_sem=rs_recv.at[(d * per + local) * lanes + sub],
                device_id={"fs": me_fs, "tp": lax.rem(me + d, tp)},
                device_id_type=MESH,
            ).wait_recv()
        c = pl.ds(pl.multiple_of(local * cols + sub * fine, fine), fine)

        @pl.loop(0, seq // 128)
        def _(i):
            r = pl.ds(pl.multiple_of(i * 128, 128), 128)
            value = parts[0, local, sub, r, :].astype(jnp.float32)
            for d in range(1, tp):
                value = value + parts[d, local, sub, r, :].astype(jnp.float32)
            value = value + fcols[r, c].astype(jnp.float32)
            total[r, c] = value
            square = value * value
            lump = square[:, 0:128]
            for j in range(1, fine // 128):
                lump = lump + square[:, j * 128 : (j + 1) * 128]
            stat[r, :] = stat[r, :] + lump

    for sub in range(lanes):
        block(0, owners[0], sub)
    stat[...] = jnp.zeros_like(stat)
    k = 1
    for hop in range(1, hops):
        start(DOWN, hop)
        settle(DOWN, hop - 1)
        for owner in (owners[-hop], owners[hop]):
            for sub in range(lanes):
                block(k, owner, sub)
            k += 1
    for copy in firsts:
        copy.wait()
    last = lax.rem(owners[hops], per)
    for j in range(1, per):
        for sub in range(lanes):
            add_up(lax.rem(last + j, per), sub)
    for sub in range(lanes):
        finish(DOWN, sub)
        block(k, owners[hops], sub)
    for sub in range(lanes):
        add_up(last, sub)

    turned = jnp.transpose(stat[...])
    stat_out[...] = jnp.broadcast_to(jnp.sum(turned, axis=0, keepdims=True), stat_out.shape)
    stats = []
    for d in range(1, tp):
        copy = pltpu.make_async_remote_copy(
            src_ref=stat_out,
            dst_ref=stat_in.at[d],
            send_sem=st_send.at[d],
            recv_sem=st_recv.at[d],
            device_id={"fs": me_fs, "tp": lax.rem(me + d, tp)},
            device_id_type=MESH,
        )
        copy.start()
        stats.append(copy)
    for copy in started:
        copy.wait_send()
    for copy in inners:
        copy.wait_send()
    if cores > 1:
        swap.wait_send()
    for d, copy in sums:
        @pl.when(d != 0)
        def _(copy=copy):
            copy.wait_send()
    for copy in stats:
        copy.wait()
    squares = stat_out[...]
    for d in range(1, tp):
        squares = squares + stat_in[d]
    factor = lax.rsqrt(squares / width + EPS)
    stat[...] = jnp.transpose(jnp.broadcast_to(factor[0:1], (128, seq)))

    @pl.loop(0, seq // 128)
    def _(i):
        r = pl.ds(pl.multiple_of(i * 128, 128), 128)
        out_ref[r, :] = (total[r, :] * stat[r, 0:1] * gout_ref[...]).astype(jnp.bfloat16)


def ring_local(order, tokens, pool_weight, pool_scale, gain_mix, gain_mlp, w_up, w_down, gain_out):
    n, tp = lax.axis_size("fs"), lax.axis_size("tp")
    rows, width = tokens.shape
    hid, cols = w_up.shape
    seq, own = rows * tp, width // tp
    bf, f32 = jnp.bfloat16, jnp.float32
    vmem = pl.BlockSpec(memory_space=pltpu.VMEM)
    dma = pltpu.SemaphoreType.DMA
    lanes = 2 if cols % 256 == 0 else 1
    return pl.pallas_call(
        functools.partial(ring_kernel, n, tp, order),
        out_shape=jax.ShapeDtypeStruct((seq, own), bf),
        in_specs=[vmem] * 8,
        out_specs=vmem,
        scratch_shapes=[
            pltpu.VMEM((pool_weight.shape[0], pool_weight.shape[1] * n, pool_weight.shape[2]), bf),
            pltpu.VMEM((hid, width), bf),
            pltpu.VMEM((hid, width), bf),
            pltpu.VMEM((rows + 2 * HALO, width), f32),
            pltpu.VMEM((rows, width), bf),
            pltpu.VMEM((seq, width), bf),
            pltpu.VMEM((seq, hid), bf),
            pltpu.VMEM((seq, own), bf),
            pltpu.VMEM((n, lanes, seq, cols // lanes), bf),
            pltpu.VMEM((tp, n // tp, lanes, seq, cols // lanes), bf),
            pltpu.VMEM((HALO, width), bf),
            pltpu.VMEM((HALO, width), bf),
            pltpu.VMEM((2, HALO, width), bf),
            pltpu.VMEM((seq, own), f32),
            pltpu.VMEM((seq, 128), f32),
            pltpu.VMEM((8, seq), f32),
            pltpu.VMEM((tp, 8, seq), f32),
            dma((12 * (n // 2) + 2 * lanes,)),
            dma((12 * (n // 2) + 2 * lanes,)),
            dma((tp,)),
            dma((tp,)),
            dma((tp,)),
            dma((tp,)),
            dma((2,)),
            dma((2,)),
            dma((n * lanes,)),
            dma((n * lanes,)),
            dma,
            dma,
            dma((tp,)),
            dma((tp,)),
        ],
        compiler_params=pltpu.CompilerParams(
            collective_id=0, has_side_effects=True, vmem_limit_bytes=63 * 1024 * 1024
        ),
    )(
        tokens, pool_weight, w_up, w_down,
        pool_scale.reshape(1, -1), gain_mix.reshape(1, -1), gain_mlp.reshape(1, -1),
        gain_out.reshape(1, -1),
    )


NEAR = ((1, 2, 3), (0, 2, 3), (3, 1, 0), (2, 1, 0))
TARGETS = ((1, 2, 3), (0, 3, 2), (3, 0, 1), (2, 1, 0))
DTARGETS = ((1, 2, 3), (0, 2, 3), (3, 1, 0), (2, 1, 0))
Y_FIRST = ((True, True), (False, False), (True, False), (True, False))
ENDS, INNER = 4, 4
UPS, DOWNS = 0, 1
HALVES = 2


def plane_kernel(
    tok_ref, pool_ref, up_ref, down_ref, scale_ref, gmix_ref, gmlp_ref, gout_ref, out_ref,
    pool_full, up_full, down_full, ext, first_all, inner_all, hidden,
    part_send, part_recv, part, y_recv, z_recv,
    before, after, edge, total, stat, stat_out, stat_in,
    pz_s, pz_r, px_s, px_r, py_s, py_r, pc_s, pc_r, wz_s, wz_r, wx_s, wx_r, halo_s, halo_r,
    f_s, f_r, d_s, d_r, y_s, y_r, z_s, z_r, st_s, st_r,
):
    rows, width = tok_ref.shape
    group = width // 4
    hid, cols = up_ref.shape
    depth = pool_ref.shape[1]
    nz, tp = 4, 4
    own_cols = width // tp
    seq = rows * tp
    most = max(ENDS, INNER)
    piece = hid // (ENDS + INNER)
    bf, f32 = jnp.bfloat16, jnp.float32
    me_fs, me = lax.axis_index("fs"), lax.axis_index("tp")
    z, x = lax.div(me_fs, 2), lax.rem(me_fs, 2)
    y, c = lax.div(me, 2), lax.rem(me, 2)
    q = lax.rem(z, 2)
    zp = z + 1 - 2 * q

    def pick(table, column):
        return lookup([row[column] for row in table], z)

    def is_end(plane):
        return (plane == 0) | (plane == nz - 1)

    def count_of(plane):
        return jnp.where(is_end(plane), ENDS, INNER)

    def base_of(plane):
        return jnp.where(is_end(plane), 0, ENDS * piece)

    def dev(z=z, x=x, y=y, c=c):
        return {"fs": z * 2 + x, "tp": y * 2 + c}

    def rc(src, dst, send, recv, to):
        return pltpu.make_async_remote_copy(
            src_ref=src, dst_ref=dst, send_sem=send, recv_sem=recv, device_id=to, device_id_type=MESH
        )

    def landed(dst, recv):
        pltpu.make_async_remote_copy(
            src_ref=dst, dst_ref=dst, send_sem=recv, recv_sem=recv, device_id=dev(x=1 - x), device_id_type=MESH
        ).wait_recv()

    barrier = pltpu.get_barrier_semaphore()
    peers = [dev(z=pick(TARGETS, k)) for k in range(3)] + [dev(x=1 - x), dev(y=1 - y), dev(c=1 - c)]
    peers.append(dev(y=1 - y, c=1 - c))
    for peer in peers:
        pl.semaphore_signal(barrier, inc=1, device_id=peer, device_id_type=MESH)
    pl.semaphore_wait(barrier, len(peers))

    always, pending = None, []

    def go(copy, condition=always):
        if condition is None:
            copy.start()
        else:
            @pl.when(condition)
            def _():
                copy.start()
        pending.append((copy, condition))

    def pool_block(g, plane, column):
        return pool_full.at[g, pl.ds(pl.multiple_of((plane * 2 + column) * depth, depth), depth), :]

    def pool_to_y(ref, plane, column):
        f = plane * 2 + column
        go(rc(ref, pool_block(me, plane, column), py_s.at[f], py_r.at[f], dev(y=1 - y)))

    def pool_to_x(ref, plane):
        go(rc(ref, pool_block(me, plane, x), px_s.at[plane], px_r.at[plane], dev(x=1 - x)))

    def pool_to_c(g, k):
        go(rc(pool_full.at[g], pool_full.at[g], pc_s.at[k], pc_r.at[k], dev(c=1 - c)))

    own_pool = pool_ref.at[me]
    for k in range(3):
        t = pick(TARGETS, k)
        go(rc(own_pool, pool_block(me, z, x), pz_s.at[t], pz_r.at[z], dev(z=t)))
    pool_to_x(own_pool, z)
    pool_to_y(own_pool, z, x)

    weights = (up_ref, down_ref)
    fulls = (up_full, down_full)

    def slot(stream, plane, p):
        return (stream * nz + plane) * most + p

    def block(stream, plane, column, p):
        return fulls[stream].at[
            pl.ds(p * piece, piece), pl.ds(pl.multiple_of((plane * 2 + column) * cols, cols), cols)
        ]

    def own_piece(stream, plane, p):
        start = pl.multiple_of(base_of(plane) + p * piece, piece)
        return weights[stream].at[pl.ds(start, piece), :]

    def some(p, plane):
        return always if p < min(ENDS, INNER) else p < count_of(plane)

    def spread_z(stream, order):
        for p, k in order:
            t = pick(DTARGETS if stream else TARGETS, k)
            go(
                rc(own_piece(stream, t, p), block(stream, z, x, p), wz_s.at[slot(stream, t, p)],
                   wz_r.at[slot(stream, z, p)], dev(z=t)),
                some(p, t),
            )

    def spread_x(stream, pieces):
        for p in pieces:
            go(
                rc(own_piece(stream, z, p), block(stream, z, x, p), wx_s.at[slot(stream, z, p)],
                   wx_r.at[slot(stream, z, p)], dev(x=1 - x)),
                some(p, z),
            )

    def guarded(condition, body):
        if condition is None:
            body()
        else:
            pl.when(condition)(body)

    def relay(stream, k, pieces):
        s = pick(NEAR, k)
        for p in pieces:
            condition = some(p, z)
            ref = block(stream, s, x, p)
            guarded(condition, lambda ref=ref, p=p: landed(ref, wz_r.at[slot(stream, s, p)]))
            go(rc(ref, ref, wx_s.at[slot(stream, s, p)], wx_r.at[slot(stream, s, p)], dev(x=1 - x)), condition)

    def from_x(stream, s, pieces):
        for p in pieces:
            ref = block(stream, s, 1 - x, p)
            guarded(some(p, z), lambda ref=ref, p=p: landed(ref, wx_r.at[slot(stream, s, p)]))

    every = range(most)
    early = range(most // 2)
    late = range(most // 2, most)
    spread_z(UPS, [(p, k) for p in every for k in range(3)])
    spread_x(UPS, early)

    step = 32 if rows % 32 == 0 else rows

    @pl.loop(0, rows // step)
    def _(i):
        r = pl.ds(pl.multiple_of(i * step, step), step)
        v = tok_ref[r, :].astype(f32)
        v = v * lax.rsqrt(jnp.mean(v * v, axis=-1, keepdims=True) + EPS) * gmix_ref[...]
        v = v.astype(bf)
        ext[pl.ds(pl.multiple_of(HALO + i * step, HALO), step), :] = v.astype(f32)

    edge[0] = ext[rows : rows + HALO, :].astype(bf)
    edge[1] = ext[HALO : 2 * HALO, :].astype(bf)
    for side, (buffer, d) in enumerate(((before, 1), (after, tp - 1))):
        to = {"fs": me_fs, "tp": lax.rem(me + d, tp)}
        go(rc(edge.at[side], buffer, halo_s.at[side], halo_r.at[side], to))

    pool_full[me, pl.ds(pl.multiple_of(me_fs * depth, depth), depth), :] = pool_ref[me, :, :]
    for k in range(3):
        s = pick(NEAR, k)
        ref = pool_block(me, s, x)
        landed(ref, pz_r.at[s])
        pool_to_x(ref, s)
        pool_to_y(ref, s, x)
    spread_x(UPS, late)
    mine = pl.ds(pl.multiple_of(me_fs * cols, cols), cols)
    for stream in (UPS, DOWNS):
        for p in range(most):
            def keep(stream=stream, p=p):
                start = pl.multiple_of(base_of(z) + p * piece, piece)
                fulls[stream][p * piece : (p + 1) * piece, mine] = weights[stream][pl.ds(start, piece), :]
            guarded(some(p, z), keep)
    landed(before, halo_r.at[0])
    landed(after, halo_r.at[1])
    offset = me * rows
    lower_open = (lax.rem(offset, SEQ_LEN) != 0).astype(f32)
    upper_open = (lax.rem(offset + rows, SEQ_LEN) != 0).astype(f32)
    ext[0:HALO, :] = before[...].astype(f32) * lower_open
    ext[rows + HALO : rows + 2 * HALO, :] = after[...].astype(f32) * upper_open
    for k in range(nz):
        s = z if k == 0 else pick(NEAR, k - 1)
        ref = pool_block(me, s, 1 - x)
        landed(ref, px_r.at[s])
        pool_to_y(ref, s, 1 - x)
    pool_to_c(me, 0)
    peer_c, peer_y, peer_yc = y * 2 + 1 - c, (1 - y) * 2 + c, (1 - y) * 2 + 1 - c
    for f in range(2 * nz):
        landed(pool_block(peer_y, f // 2, f % 2), py_r.at[f])
    pool_to_c(peer_y, 1)
    landed(pool_full.at[peer_c], pc_r.at[0])
    landed(pool_full.at[peer_yc], pc_r.at[1])

    def rows_of(s, t):
        return pl.ds(pl.multiple_of(s * seq + t * rows, rows), rows)

    my_rows = rows_of(q, me)
    position = lax.rem(offset + lax.broadcasted_iota(jnp.int32, (rows, 1), 0), SEQ_LEN)
    for index, reach in enumerate(WINDOWS):
        half = reach // 2
        g = slice(index * group, (index + 1) * group)
        level = ext[:, g]
        own = level[HALO : HALO + rows]
        shift = 1
        while shift < reach:
            level = level + pltpu.roll(level, shift, 0)
            shift *= 2
        if half > 1:
            level = pltpu.roll(level, rows + 2 * HALO - (half - 1), 0)
        window = level[HALO : HALO + rows]
        counts = (jnp.minimum(position + half, SEQ_LEN) - jnp.maximum(position - half, 0)).astype(f32)
        pooled = (window / counts - own).astype(bf)
        mixed = jnp.dot(pooled, pool_full[index], preferred_element_type=f32)
        first_all[my_rows, g] = (tok_ref[:, g].astype(f32) + mixed * scale_ref[:, g]).astype(bf)

    part_rows = rows // HALVES

    def first_part(s, t, h):
        return first_all.at[pl.ds(pl.multiple_of(s * seq + t * rows + h * part_rows, part_rows), part_rows), :]

    def share(s, t, k, to, h):
        ref = first_part(s, t, h)
        go(rc(ref, ref, f_s.at[k * HALVES + h], f_r.at[k * HALVES + h], to))

    def shared(s, t, k, h):
        landed(first_part(s, t, h), f_r.at[k * HALVES + h])

    halves = range(HALVES)
    for h in halves:
        share(q, me, 0, dev(z=zp), h)
        share(q, me, 1, dev(y=1 - y), h)
        share(q, me, 3, dev(c=1 - c), h)

    def groups(s, yy):
        return s * seq + yy * 2 * rows

    def norm(begin):
        @pl.loop(0, 2 * rows // step)
        def _(i):
            r = pl.ds(pl.multiple_of(begin + i * step, step), step)
            v = first_all[r, :].astype(f32)
            v = v * lax.rsqrt(jnp.mean(v * v, axis=-1, keepdims=True) + EPS) * gmlp_ref[...]
            inner_all[r, :] = v.astype(bf)

    def up(begin, lo, hi):
        g = pl.ds(pl.multiple_of(begin, 2 * rows), 2 * rows)

        @pl.loop(lo, hi)
        def _(j):
            h = pl.ds(pl.multiple_of(j * piece, piece), piece)
            pre = lax.dot_general(
                inner_all[g, :], up_full[h, :], (((1,), (1,)), ((), ())), preferred_element_type=f32
            )
            hidden[g, h] = jnp.square(jnp.maximum(pre, 0.0)).astype(bf)

    def pull(pieces):
        for p in pieces:
            for k in range(3):
                relay(UPS, k, (p,))

    def ready(pieces):
        for s in range(nz):
            from_x(UPS, s, pieces)

    def forward_z():
        for h in halves:
            shared(1 - q, me, 0, h)
            share(1 - q, me, 2, dev(y=1 - y), h)
            share(1 - q, me, 4, dev(c=1 - c), h)

    def forward_y(s, k, kc):
        for h in halves:
            shared(s, peer_y, k, h)
            share(s, peer_y, kc, dev(c=1 - c), h)

    def from_c(s, t, k):
        for h in halves:
            shared(s, t, k, h)

    g0, g1, g2, g3 = groups(q, y), groups(q, 1 - y), groups(1 - q, y), groups(1 - q, 1 - y)
    quarter = most // 4
    p0, p1, p2, p3 = [range(k * quarter, most if k == 3 else (k + 1) * quarter) for k in range(4)]
    half = 2 * quarter
    pull(p0)
    from_c(q, peer_c, 3)
    norm(g0)
    pull(p1)
    ready(p0)
    ready(p1)
    up(g0, 0, half)
    spread_x(DOWNS, every)
    forward_y(q, 1, 5)
    from_c(q, peer_yc, 5)
    norm(g1)
    up(g1, 0, half)
    pull(p2)
    spread_z(DOWNS, [(p, k) for k in range(3) for p in every])
    forward_z()
    pull(p3)
    from_c(1 - q, peer_c, 4)
    norm(g2)
    up(g2, 0, half)
    ready(p2)
    relay(DOWNS, 0, every)
    ready(p3)
    up(g0, half, count_of(z))
    up(g1, half, count_of(z))
    up(g2, half, count_of(z))
    forward_y(1 - q, 2, 6)
    from_c(1 - q, peer_yc, 6)
    norm(g3)
    up(g3, 0, count_of(z))
    first_sends = list(pending)
    pending.clear()

    chunk = 2 * rows
    orow = pl.ds(pl.multiple_of(q * seq, seq), seq)
    prow = pl.ds(pl.multiple_of((1 - q) * seq, seq), seq)
    fine = 128

    def unit(i, j):
        plane = jnp.where(z < 2, i, nz - 1 - i)
        column = x if j == 0 else 1 - x
        return plane, column, (i // 2) * 2 + j, i * 2 + j

    def each(begin, size, body):
        @pl.loop(0, size // fine)
        def _(i):
            body(pl.ds(pl.multiple_of(begin + i * fine, fine), fine), pl.ds(pl.multiple_of(i * fine, fine), fine))

    def send_part(i, j):
        plane, column, s, u = unit(i, j)
        go(rc(part_send.at[s], part_recv.at[s], d_s.at[u], d_r.at[u], dev(c=1 - c)), lax.rem(plane, 2) != c)

    def multiply(theirs, deep, cc, slots):
        def all_rows(theirs, deep):
            @pl.loop(0, 2 * seq // chunk)
            def _(k):
                r = pl.ds(pl.multiple_of(k * chunk, chunk), chunk)
                value = jnp.dot(hidden[r, 0:deep], down_full[0:deep, cc], preferred_element_type=f32)
                for n, s in enumerate(slots):
                    lane = slice(n * cols, (n + 1) * cols)
                    if theirs:
                        part_send[s, r, :] = value[:, lane].astype(bf)
                    else:
                        part[s, r, :] = value[:, lane]

        pl.when(theirs)(lambda: all_rows(True, deep))
        pl.when(jnp.logical_not(theirs))(lambda: all_rows(False, deep))

    def by_depth(body):
        if ENDS == INNER:
            body(ENDS * piece)
        else:
            pl.when(is_end(z))(lambda: body(ENDS * piece))
            pl.when(jnp.logical_not(is_end(z)))(lambda: body(INNER * piece))

    def product(i, j):
        plane, column, s, u = unit(i, j)
        cc = pl.ds(pl.multiple_of((plane * 2 + column) * cols, cols), cols)
        if j == 1:
            from_x(DOWNS, plane, every)
        by_depth(lambda deep: multiply(lax.rem(plane, 2) != c, deep, cc, (s,)))
        send_part(i, j)

    def wide_product(i):
        plane = jnp.where(z < 2, i, nz - 1 - i)
        cc = pl.ds(pl.multiple_of(plane * 2 * cols, 2 * cols), 2 * cols)
        from_x(DOWNS, plane, every)
        slots = ((i // 2) * 2 + x, (i // 2) * 2 + 1 - x)
        by_depth(lambda deep: multiply(lax.rem(plane, 2) != c, deep, cc, slots))
        for j in (0, 1):
            send_part(i, j)

    def stage1(i, j):
        plane, column, s, u = unit(i, j)
        ours = lax.rem(plane, 2) == c
        home = lax.div(plane, 2) == y

        def fold(begin, size, keep):
            def body(r, _):
                value = part[s, r, :] + part_recv[s, r, :].astype(f32)
                if keep:
                    part[s, r, :] = value
                else:
                    part_recv[s, r, :] = value.astype(bf)
            each(begin, size, body)

        @pl.when(ours)
        def _():
            landed(part_recv.at[s], d_r.at[u])
            if not Y_FIRST[i][j]:
                fold((1 - q) * seq, seq, False)

        if Y_FIRST[i][j]:
            pl.when(ours & home)(lambda: fold(0, 2 * seq, True))
            pl.when(ours & jnp.logical_not(home))(lambda: fold(0, 2 * seq, False))
            go(rc(part_recv.at[s], y_recv.at[j], y_s.at[u], y_r.at[u], dev(y=1 - y)), ours & jnp.logical_not(home))
        else:
            go(rc(part_recv.at[s, prow, :], z_recv.at[s], z_s.at[u], z_r.at[u], dev(z=zp)), ours)
            pl.when(ours)(lambda: fold(q * seq, seq, True))

    def stage2(i, j):
        plane, column, s, u = unit(i, j)
        ours = lax.rem(plane, 2) == c
        home = lax.div(plane, 2) == y
        if Y_FIRST[i][j]:
            @pl.when(ours & home)
            def _():
                landed(y_recv.at[j], y_r.at[u])

                def out(r, _):
                    y_recv[j, r, :] = (part[s, r, :] + y_recv[j, r, :].astype(f32)).astype(bf)
                each((1 - q) * seq, seq, out)

            go(rc(y_recv.at[j, prow, :], z_recv.at[s], z_s.at[u], z_r.at[u], dev(z=zp)), ours & home)

            @pl.when(ours & home)
            def _():
                def kept(r, _):
                    part[s, r, :] = part[s, r, :] + y_recv[j, r, :].astype(f32)
                each(q * seq, seq, kept)
        else:
            @pl.when(ours)
            def _():
                landed(z_recv.at[s], z_r.at[u])

            @pl.when(ours & jnp.logical_not(home))
            def _():
                def out(r, l):
                    part_recv[s, r, :] = (part[s, r, :] + z_recv[s, l, :].astype(f32)).astype(bf)
                each(q * seq, seq, out)

            go(rc(part_recv.at[s, orow, :], y_recv.at[j, orow, :], y_s.at[u], y_r.at[u], dev(y=1 - y)),
               ours & jnp.logical_not(home))

            @pl.when(ours & home)
            def _():
                def kept(r, l):
                    part[s, r, :] = part[s, r, :] + z_recv[s, l, :].astype(f32)
                each(q * seq, seq, kept)

    def stage3(i, j):
        plane, column, s, u = unit(i, j)

        @pl.when(plane == me)
        def _():
            if Y_FIRST[i][j]:
                landed(z_recv.at[s], z_r.at[u])
            else:
                landed(y_recv.at[j, orow, :], y_r.at[u])
            here = pl.ds(pl.multiple_of(column * cols, cols), cols)
            cc = pl.ds(pl.multiple_of(me * own_cols + column * cols, cols), cols)

            def body(r, l):
                more = z_recv[s, l, :] if Y_FIRST[i][j] else y_recv[j, r, :]
                value = part[s, r, :] + more.astype(f32) + first_all[r, cc].astype(f32)
                total[l, here] = value
                square = value * value
                lump = square[:, 0:128]
                for k in range(1, cols // 128):
                    lump = lump + square[:, k * 128 : (k + 1) * 128]
                stat[l, :] = stat[l, :] + lump
            each(q * seq, seq, body)

    stat[...] = jnp.zeros_like(stat)
    both = (0, 1)

    def run(body, i):
        for j in both:
            body(i, j)

    def drain():
        for copy, condition in pending:
            guarded(condition, copy.wait_send)
        pending.clear()

    wide_product(0)
    relay(DOWNS, 1, every)
    wide_product(1)
    run(stage1, 0)
    run(stage1, 1)
    wide_product(2)
    run(stage1, 2)
    relay(DOWNS, 2, every)
    run(product, 3)
    run(stage2, 1)
    run(stage1, 3)
    for copy, condition in first_sends:
        guarded(condition, copy.wait_send)
    run(stage2, 0)
    run(stage2, 2)
    run(stage2, 3)
    run(stage3, 0)
    run(stage3, 1)
    run(stage3, 2)
    run(stage3, 3)

    turned = jnp.transpose(stat[...])
    stat_out[...] = jnp.broadcast_to(jnp.sum(turned, axis=0, keepdims=True), stat_out.shape)
    for d in range(1, tp):
        to = {"fs": me_fs, "tp": lax.rem(me + d, tp)}
        go(rc(stat_out, stat_in.at[d], st_s.at[d], st_r.at[d], to))
    drain()
    squares = stat_out[...]
    for d in range(1, tp):
        landed(stat_in.at[d], st_r.at[d])
        squares = squares + stat_in[d]
    factor = lax.rsqrt(squares / width + EPS)
    stat[...] = jnp.transpose(jnp.broadcast_to(factor[0:1], (128, seq)))

    @pl.loop(0, seq // 128)
    def _(i):
        r = pl.ds(pl.multiple_of(i * 128, 128), 128)
        out_ref[r, :] = (total[r, :] * stat[r, 0:1] * gout_ref[...]).astype(bf)


def plane_local(tokens, pool_weight, pool_scale, gain_mix, gain_mlp, w_up, w_down, gain_out):
    n, tp = lax.axis_size("fs"), lax.axis_size("tp")
    rows, width = tokens.shape
    hid, cols = w_up.shape
    seq, own = rows * tp, width // tp
    bf, f32 = jnp.bfloat16, jnp.float32
    vmem = pl.BlockSpec(memory_space=pltpu.VMEM)
    dma = pltpu.SemaphoreType.DMA
    most = max(ENDS, INNER)
    deep = hid // (ENDS + INNER) * most
    lots = 2 * 4 * most
    return pl.pallas_call(
        plane_kernel,
        out_shape=jax.ShapeDtypeStruct((seq, own), bf),
        in_specs=[vmem] * 8,
        out_specs=vmem,
        scratch_shapes=[
            pltpu.VMEM((pool_weight.shape[0], pool_weight.shape[1] * n, pool_weight.shape[2]), bf),
            pltpu.VMEM((deep, width), bf),
            pltpu.VMEM((deep, width), bf),
            pltpu.VMEM((rows + 2 * HALO, width), f32),
            pltpu.VMEM((2 * seq, width), bf),
            pltpu.VMEM((2 * seq, width), bf),
            pltpu.VMEM((2 * seq, deep), bf),
            pltpu.VMEM((4, 2 * seq, cols), bf),
            pltpu.VMEM((4, 2 * seq, cols), bf),
            pltpu.VMEM((4, 2 * seq, cols), f32),
            pltpu.VMEM((2, 2 * seq, cols), bf),
            pltpu.VMEM((4, seq, cols), bf),
            pltpu.VMEM((HALO, width), bf),
            pltpu.VMEM((HALO, width), bf),
            pltpu.VMEM((2, HALO, width), bf),
            pltpu.VMEM((seq, own), f32),
            pltpu.VMEM((seq, 128), f32),
            pltpu.VMEM((8, seq), f32),
            pltpu.VMEM((tp, 8, seq), f32),
            dma((4,)), dma((4,)), dma((4,)), dma((4,)), dma((8,)), dma((8,)), dma((2,)), dma((2,)),
            dma((lots,)), dma((lots,)), dma((lots,)), dma((lots,)),
            dma((2,)), dma((2,)),
            dma((7 * HALVES,)), dma((7 * HALVES,)),
            dma((8,)), dma((8,)), dma((8,)), dma((8,)), dma((8,)), dma((8,)),
            dma((tp,)), dma((tp,)),
        ],
        compiler_params=pltpu.CompilerParams(
            collective_id=0, has_side_effects=True, vmem_limit_bytes=63 * 1024 * 1024
        ),
    )(
        tokens, pool_weight, w_up, w_down,
        pool_scale.reshape(1, -1), gain_mix.reshape(1, -1), gain_mlp.reshape(1, -1),
        gain_out.reshape(1, -1),
    )


def grid_width(mesh):
    n = mesh.shape["fs"]
    try:
        line = mesh.devices.reshape(n, -1)[:, 0]
        nx = len({d.coords[0] for d in line})
        if n % nx == 0:
            return nx
    except AttributeError:
        pass
    return 2 if n % 2 == 0 else 1


def solution(mesh):
    n, tp, nx = mesh.shape["fs"], mesh.shape["tp"], grid_width(mesh)
    if nx == 2 and n == 8 and tp == 4:
        body = plane_local
    else:
        body = functools.partial(ring_local, ring_order(n, nx))
    return jax.shard_map(
        body,
        mesh=mesh,
        in_specs=(
            P(("fs", "tp"), None),
            P(None, "fs", None),
            P(),
            P(),
            P(),
            P("tp", "fs"),
            P("tp", "fs"),
            P("tp"),
        ),
        out_specs=P("fs", "tp"),
        check_vma=False,
    )
```

```python
import functools

import jax
import jax.numpy as jnp
from jax import lax
from jax.experimental import pallas as pl
from jax.experimental.pallas import tpu as pltpu
from jax.sharding import PartitionSpec as P

SEQ_LEN = 1024
EPS = 1e-06
WINDOWS = (2, 4, 8, 16)
HALO = 16
MESH = pl.DeviceIdType.MESH
POOL, UP, DOWN = 0, 1, 2


def ring_order(n, nx):
    nz = n // nx
    if nx < 2 or nz < 2 or nz % 2:
        return list(range(n))
    order = []
    for z in range(nz):
        xs = list(range(1, nx))
        order += [z * nx + x for x in (xs if z % 2 == 0 else xs[::-1])]
    return order + [z * nx for z in range(nz - 1, -1, -1)]


def lookup(table, index):
    value = jnp.int32(table[0])
    for i in range(1, len(table)):
        value = jnp.where(index == i, jnp.int32(table[i]), value)
    return value


def ring_kernel(
    n, tp, order, tok_ref, pool_ref, up_ref, down_ref, scale_ref, gmix_ref, gmlp_ref,
    gout_ref, out_ref,
    pool_full, up_full, down_full, ext, first, inner_all, hidden, fcols, blocks, parts,
    before, after, edge, total, stat, stat_out, stat_in,
    ring_send, ring_recv, in_send, in_recv, fc_send, fc_recv, halo_send, halo_recv, rs_send, rs_recv,
    pair_send, pair_recv, st_send, st_recv,
):
    rows, width = tok_ref.shape
    group = width // 4
    hid, cols = up_ref.shape
    depth = pool_ref.shape[1]
    own_cols = width // tp
    per = n // tp
    seq = rows * tp
    me_fs, me = lax.axis_index("fs"), lax.axis_index("tp")
    place_of = [order.index(i) for i in range(n)]
    place = lookup(place_of, me_fs)

    def at(offset):
        return lookup(order, lax.rem(place + offset + 2 * n, n))

    owners = {0: me_fs}
    for d in range(1, n // 2 + 1):
        owners[d] = at(d)
        owners[-d] = at(-d)
    right, left = owners[1], owners[-1]

    barrier = pltpu.get_barrier_semaphore()
    for peer in (right, left):
        pl.semaphore_signal(barrier, inc=1, device_id={"fs": peer, "tp": me}, device_id_type=MESH)
    for d in range(1, tp):
        pl.semaphore_signal(
            barrier, inc=1, device_id={"fs": me_fs, "tp": lax.rem(me + d, tp)}, device_id_type=MESH
        )
    pl.semaphore_wait(barrier, 2 + tp - 1)

    hops = n // 2
    cores = 2 if tp % 2 == 0 else 1
    core = lax.rem(me, cores)
    lanes = 2 if cols % 256 == 0 else 1
    fine = cols // lanes

    def view(stream, full, owner, piece, sub=None):
        if stream == POOL:
            ref = pool_full if full else pool_ref
            half = ref.shape[0] // (2 * cores)
            r = pl.ds(pl.multiple_of(owner * depth, depth), depth) if full else slice(None)
            return ref.at[pl.ds((core * 2 + piece) * half, half), r, :]
        ref = (up_full if full else up_ref) if stream == UP else (down_full if full else down_ref)
        half = hid // 2
        c = pl.ds(pl.multiple_of(owner * cols, cols), cols) if full else slice(None)
        if sub is not None:
            c = pl.ds(pl.multiple_of(owner * cols + sub * fine, fine), fine)
        return ref.at[pl.ds(piece * half, half), c]

    def count(side, piece):
        return hops if piece == side else hops - 1

    def slot(stream, side, piece, hop, sub):
        if sub:
            return 12 * hops + side * (lanes - 1) + sub - 1
        return ((stream * 2 + side) * 2 + piece) * hops + hop

    def subs(stream, hop):
        return range(lanes) if stream == DOWN and hop == hops - 1 and hop > 0 else (None,)

    def ring(stream, side, piece, hop, sub):
        owner = owners[-hop] if side == 0 else owners[hop]
        return pltpu.make_async_remote_copy(
            src_ref=view(stream, hop > 0, owner, piece, sub),
            dst_ref=view(stream, True, owner, piece, sub),
            send_sem=ring_send.at[slot(stream, side, piece, hop, sub)],
            recv_sem=ring_recv.at[slot(stream, side, piece, hop, sub)],
            device_id={"fs": right if side == 0 else left, "tp": me},
            device_id_type=MESH,
        )

    started = []

    def arrived(stream, side, piece, hop, sub=None):
        owner = owners[-hop - 1] if side == 0 else owners[hop + 1]
        pltpu.make_async_remote_copy(
            src_ref=view(stream, True, owner, piece, sub),
            dst_ref=view(stream, True, owner, piece, sub),
            send_sem=ring_send.at[slot(stream, side, piece, hop, sub)],
            recv_sem=ring_recv.at[slot(stream, side, piece, hop, sub)],
            device_id={"fs": right if side == 0 else left, "tp": me},
            device_id_type=MESH,
        ).wait_recv()

    def start(stream, hop, which=(0, 1)):
        for w in which:
            for side in (0, 1):
                piece = side if w == 0 else 1 - side
                if hop < count(side, piece):
                    if hop > 0:
                        arrived(stream, side, piece, hop - 1)
                    for sub in subs(stream, hop):
                        copy = ring(stream, side, piece, hop, sub)
                        copy.start()
                        started.append(copy)

    def finish(stream, sub=None):
        for side in (0, 1):
            arrived(stream, side, side, hops - 1, sub)

    def settle(stream, hop):
        if hop == hops - 2:
            for side in (0, 1):
                arrived(stream, side, 1 - side, hop)

    start(POOL, 0)
    start(UP, 0, (0,))

    step = 32 if rows % 32 == 0 else rows

    @pl.loop(0, rows // step)
    def _(i):
        r = pl.ds(pl.multiple_of(i * step, step), step)
        x = tok_ref[r, :].astype(jnp.float32)
        y = x * lax.rsqrt(jnp.mean(x * x, axis=-1, keepdims=True) + EPS) * gmix_ref[...]
        y = y.astype(jnp.bfloat16)
        ext[pl.ds(pl.multiple_of(HALO + i * step, HALO), step), :] = y.astype(jnp.float32)

    edge[0] = ext[rows : rows + HALO, :].astype(jnp.bfloat16)
    edge[1] = ext[HALO : 2 * HALO, :].astype(jnp.bfloat16)
    halos = []
    for side, (buffer, d) in enumerate(((before, 1), (after, tp - 1))):
        copy = pltpu.make_async_remote_copy(
            src_ref=edge.at[side],
            dst_ref=buffer,
            send_sem=halo_send.at[side],
            recv_sem=halo_recv.at[side],
            device_id={"fs": me_fs, "tp": lax.rem(me + d, tp)},
            device_id_type=MESH,
        )
        copy.start()
        halos.append(copy)

    start(POOL, 1)
    start(UP, 0, (1,))
    for hop in range(2, hops):
        start(POOL, hop)
    share = pl.ds(core * (pool_full.shape[0] // cores), pool_full.shape[0] // cores)
    pool_full[share, pl.ds(pl.multiple_of(me_fs * depth, depth), depth), :] = pool_ref[share, :, :]
    mine = pl.ds(pl.multiple_of(me_fs * cols, cols), cols)
    up_full[:, mine] = up_ref[...]
    down_full[:, mine] = down_ref[...]
    for copy in halos:
        copy.wait()
    offset = me * rows
    lower_open = (lax.rem(offset, SEQ_LEN) != 0).astype(jnp.float32)
    upper_open = (lax.rem(offset + rows, SEQ_LEN) != 0).astype(jnp.float32)
    ext[0:HALO, :] = before[...].astype(jnp.float32) * lower_open
    ext[rows + HALO : rows + 2 * HALO, :] = after[...].astype(jnp.float32) * upper_open
    start(UP, 1)
    settle(POOL, hops - 2)
    finish(POOL)
    if cores > 1:
        swap = pltpu.make_async_remote_copy(
            src_ref=pool_full.at[share],
            dst_ref=pool_full.at[share],
            send_sem=pair_send,
            recv_sem=pair_recv,
            device_id={"fs": me_fs, "tp": me + 1 - 2 * core},
            device_id_type=MESH,
        )
        swap.start()
        other = pl.ds((1 - core) * (pool_full.shape[0] // cores), pool_full.shape[0] // cores)
        pltpu.make_async_remote_copy(
            src_ref=pool_full.at[other],
            dst_ref=pool_full.at[other],
            send_sem=pair_send,
            recv_sem=pair_recv,
            device_id={"fs": me_fs, "tp": me + 1 - 2 * core},
            device_id_type=MESH,
        ).wait_recv()

    position = lax.rem(offset + lax.broadcasted_iota(jnp.int32, (rows, 1), 0), SEQ_LEN)
    for index, reach in enumerate(WINDOWS):
        half = reach // 2
        c = slice(index * group, (index + 1) * group)
        level = ext[:, c]
        own = level[HALO : HALO + rows]
        shift = 1
        while shift < reach:
            level = level + pltpu.roll(level, shift, 0)
            shift *= 2
        if half > 1:
            level = pltpu.roll(level, rows + 2 * HALO - (half - 1), 0)
        window = level[HALO : HALO + rows]
        counts = (jnp.minimum(position + half, SEQ_LEN) - jnp.maximum(position - half, 0)).astype(jnp.float32)
        pooled = (window / counts - own).astype(jnp.bfloat16)
        mixed = jnp.dot(pooled, pool_full[index], preferred_element_type=jnp.float32)
        first[:, c] = (tok_ref[:, c].astype(jnp.float32) + mixed * scale_ref[:, c]).astype(jnp.bfloat16)
    for hop in range(2, 3):
        if hop < hops:
            start(UP, hop)

    @pl.loop(0, rows // step)
    def _(i):
        r = pl.ds(pl.multiple_of(i * step, step), step)
        x = first[r, :].astype(jnp.float32)
        y = x * lax.rsqrt(jnp.mean(x * x, axis=-1, keepdims=True) + EPS) * gmlp_ref[...]
        inner_all[pl.ds(pl.multiple_of(me * rows + i * step, step), step), :] = y.astype(jnp.bfloat16)

    my_rows = pl.ds(pl.multiple_of(me * rows, rows), rows)
    inners, firsts = [], []
    for d in range(1, tp):
        peer = lax.rem(me + d, tp)
        copy = pltpu.make_async_remote_copy(
            src_ref=inner_all.at[my_rows, :],
            dst_ref=inner_all.at[my_rows, :],
            send_sem=in_send.at[d],
            recv_sem=in_recv.at[d],
            device_id={"fs": me_fs, "tp": peer},
            device_id_type=MESH,
        )
        copy.start()
        inners.append(copy)
    for d in range(1, tp):
        peer = lax.rem(me + d, tp)
        copy = pltpu.make_async_remote_copy(
            src_ref=first.at[:, pl.ds(pl.multiple_of(peer * own_cols, own_cols), own_cols)],
            dst_ref=fcols.at[my_rows, :],
            send_sem=fc_send.at[d],
            recv_sem=fc_recv.at[d],
            device_id={"fs": me_fs, "tp": peer},
            device_id_type=MESH,
        )
        copy.start()
        firsts.append(copy)
    fcols[my_rows, :] = first[:, pl.ds(pl.multiple_of(me * own_cols, own_cols), own_cols)]

    for hop in range(3, hops):
        start(UP, hop)
    settle(UP, hops - 2)
    start(DOWN, 0)
    finish(UP)
    for d in range(1, tp):
        source = pl.ds(pl.multiple_of(lax.rem(me + tp - d, tp) * rows, rows), rows)
        pltpu.make_async_remote_copy(
            src_ref=inner_all.at[source, :],
            dst_ref=inner_all.at[source, :],
            send_sem=in_send.at[d],
            recv_sem=in_recv.at[d],
            device_id={"fs": me_fs, "tp": lax.rem(me + d, tp)},
            device_id_type=MESH,
        ).wait_recv()

    tile = min(256, hid)

    @pl.loop(0, hid // tile)
    def _(j):
        h = pl.ds(pl.multiple_of(j * tile, tile), tile)
        pre = lax.dot_general(
            inner_all[...], up_full[h, :], (((1,), (1,)), ((), ())), preferred_element_type=jnp.float32
        )
        hidden[:, h] = jnp.square(jnp.maximum(pre, 0.0)).astype(jnp.bfloat16)

    sums = []
    part = min(512, seq)

    def block(k, owner, sub):
        c = pl.ds(pl.multiple_of(owner * cols + sub * fine, fine), fine)

        @pl.loop(0, seq // part)
        def _(i):
            r = pl.ds(pl.multiple_of(i * part, part), part)
            blocks[k, sub, r, :] = jnp.dot(
                hidden[r, :], down_full[:, c], preferred_element_type=jnp.float32
            ).astype(jnp.bfloat16)

        dest = owner // per
        d = lax.rem(dest - me + tp, tp)
        local = lax.rem(owner, per)
        copy = pltpu.make_async_remote_copy(
            src_ref=blocks.at[k, sub],
            dst_ref=parts.at[d, local, sub],
            send_sem=rs_send.at[k * lanes + sub],
            recv_sem=rs_recv.at[(d * per + local) * lanes + sub],
            device_id={"fs": me_fs, "tp": dest},
            device_id_type=MESH,
        )

        @pl.when(d == 0)
        def _():
            parts[0, local, sub] = blocks[k, sub]

        @pl.when(d != 0)
        def _():
            copy.start()

        sums.append((d, copy))

    def add_up(local, sub):
        for d in range(1, tp):
            pltpu.make_async_remote_copy(
                src_ref=blocks.at[0, sub],
                dst_ref=parts.at[d, local, sub],
                send_sem=rs_send.at[0],
                recv_sem=rs_recv.at[(d * per + local) * lanes + sub],
                device_id={"fs": me_fs, "tp": lax.rem(me + d, tp)},
                device_id_type=MESH,
            ).wait_recv()
        c = pl.ds(pl.multiple_of(local * cols + sub * fine, fine), fine)

        @pl.loop(0, seq // 128)
        def _(i):
            r = pl.ds(pl.multiple_of(i * 128, 128), 128)
            value = parts[0, local, sub, r, :].astype(jnp.float32)
            for d in range(1, tp):
                value = value + parts[d, local, sub, r, :].astype(jnp.float32)
            value = value + fcols[r, c].astype(jnp.float32)
            total[r, c] = value
            square = value * value
            lump = square[:, 0:128]
            for j in range(1, fine // 128):
                lump = lump + square[:, j * 128 : (j + 1) * 128]
            stat[r, :] = stat[r, :] + lump

    for sub in range(lanes):
        block(0, owners[0], sub)
    stat[...] = jnp.zeros_like(stat)
    k = 1
    for hop in range(1, hops):
        start(DOWN, hop)
        settle(DOWN, hop - 1)
        for owner in (owners[-hop], owners[hop]):
            for sub in range(lanes):
                block(k, owner, sub)
            k += 1
    for copy in firsts:
        copy.wait()
    last = lax.rem(owners[hops], per)
    for j in range(1, per):
        for sub in range(lanes):
            add_up(lax.rem(last + j, per), sub)
    for sub in range(lanes):
        finish(DOWN, sub)
        block(k, owners[hops], sub)
    for sub in range(lanes):
        add_up(last, sub)

    turned = jnp.transpose(stat[...])
    stat_out[...] = jnp.broadcast_to(jnp.sum(turned, axis=0, keepdims=True), stat_out.shape)
    stats = []
    for d in range(1, tp):
        copy = pltpu.make_async_remote_copy(
            src_ref=stat_out,
            dst_ref=stat_in.at[d],
            send_sem=st_send.at[d],
            recv_sem=st_recv.at[d],
            device_id={"fs": me_fs, "tp": lax.rem(me + d, tp)},
            device_id_type=MESH,
        )
        copy.start()
        stats.append(copy)
    for copy in started:
        copy.wait_send()
    for copy in inners:
        copy.wait_send()
    if cores > 1:
        swap.wait_send()
    for d, copy in sums:
        @pl.when(d != 0)
        def _(copy=copy):
            copy.wait_send()
    for copy in stats:
        copy.wait()
    squares = stat_out[...]
    for d in range(1, tp):
        squares = squares + stat_in[d]
    factor = lax.rsqrt(squares / width + EPS)
    stat[...] = jnp.transpose(jnp.broadcast_to(factor[0:1], (128, seq)))

    @pl.loop(0, seq // 128)
    def _(i):
        r = pl.ds(pl.multiple_of(i * 128, 128), 128)
        out_ref[r, :] = (total[r, :] * stat[r, 0:1] * gout_ref[...]).astype(jnp.bfloat16)


def ring_local(order, tokens, pool_weight, pool_scale, gain_mix, gain_mlp, w_up, w_down, gain_out):
    n, tp = lax.axis_size("fs"), lax.axis_size("tp")
    rows, width = tokens.shape
    hid, cols = w_up.shape
    seq, own = rows * tp, width // tp
    bf, f32 = jnp.bfloat16, jnp.float32
    vmem = pl.BlockSpec(memory_space=pltpu.VMEM)
    dma = pltpu.SemaphoreType.DMA
    lanes = 2 if cols % 256 == 0 else 1
    return pl.pallas_call(
        functools.partial(ring_kernel, n, tp, order),
        out_shape=jax.ShapeDtypeStruct((seq, own), bf),
        in_specs=[vmem] * 8,
        out_specs=vmem,
        scratch_shapes=[
            pltpu.VMEM((pool_weight.shape[0], pool_weight.shape[1] * n, pool_weight.shape[2]), bf),
            pltpu.VMEM((hid, width), bf),
            pltpu.VMEM((hid, width), bf),
            pltpu.VMEM((rows + 2 * HALO, width), f32),
            pltpu.VMEM((rows, width), bf),
            pltpu.VMEM((seq, width), bf),
            pltpu.VMEM((seq, hid), bf),
            pltpu.VMEM((seq, own), bf),
            pltpu.VMEM((n, lanes, seq, cols // lanes), bf),
            pltpu.VMEM((tp, n // tp, lanes, seq, cols // lanes), bf),
            pltpu.VMEM((HALO, width), bf),
            pltpu.VMEM((HALO, width), bf),
            pltpu.VMEM((2, HALO, width), bf),
            pltpu.VMEM((seq, own), f32),
            pltpu.VMEM((seq, 128), f32),
            pltpu.VMEM((8, seq), f32),
            pltpu.VMEM((tp, 8, seq), f32),
            dma((12 * (n // 2) + 2 * lanes,)),
            dma((12 * (n // 2) + 2 * lanes,)),
            dma((tp,)),
            dma((tp,)),
            dma((tp,)),
            dma((tp,)),
            dma((2,)),
            dma((2,)),
            dma((n * lanes,)),
            dma((n * lanes,)),
            dma,
            dma,
            dma((tp,)),
            dma((tp,)),
        ],
        compiler_params=pltpu.CompilerParams(
            collective_id=0, has_side_effects=True, vmem_limit_bytes=63 * 1024 * 1024
        ),
    )(
        tokens, pool_weight, w_up, w_down,
        pool_scale.reshape(1, -1), gain_mix.reshape(1, -1), gain_mlp.reshape(1, -1),
        gain_out.reshape(1, -1),
    )


NEAR = ((1, 2, 3), (0, 2, 3), (3, 1, 0), (2, 1, 0))
TARGETS = ((1, 2, 3), (0, 3, 2), (3, 0, 1), (2, 1, 0))
DTARGETS = ((1, 2, 3), (0, 2, 3), (3, 1, 0), (2, 1, 0))
Y_FIRST = ((True, True), (False, False), (True, False), (True, False))
ENDS, INNER = 4, 4
UPS, DOWNS = 0, 1
HALVES = 2


def plane_kernel(
    tok_ref, pool_ref, up_ref, down_ref, scale_ref, gmix_ref, gmlp_ref, gout_ref, out_ref,
    pool_full, up_full, down_full, ext, first_all, inner_all, hidden,
    part_send, part_recv, part, y_recv, z_recv,
    before, after, edge, total, stat, stat_out, stat_in,
    pz_s, pz_r, px_s, px_r, py_s, py_r, pc_s, pc_r, wz_s, wz_r, wx_s, wx_r, halo_s, halo_r,
    f_s, f_r, d_s, d_r, y_s, y_r, z_s, z_r, st_s, st_r,
):
    rows, width = tok_ref.shape
    group = width // 4
    hid, cols = up_ref.shape
    depth = pool_ref.shape[1]
    nz, tp = 4, 4
    own_cols = width // tp
    seq = rows * tp
    most = max(ENDS, INNER)
    piece = hid // (ENDS + INNER)
    bf, f32 = jnp.bfloat16, jnp.float32
    me_fs, me = lax.axis_index("fs"), lax.axis_index("tp")
    z, x = lax.div(me_fs, 2), lax.rem(me_fs, 2)
    y, c = lax.div(me, 2), lax.rem(me, 2)
    q = lax.rem(z, 2)
    zp = z + 1 - 2 * q

    def pick(table, column):
        return lookup([row[column] for row in table], z)

    def is_end(plane):
        return (plane == 0) | (plane == nz - 1)

    def count_of(plane):
        return jnp.where(is_end(plane), ENDS, INNER)

    def base_of(plane):
        return jnp.where(is_end(plane), 0, ENDS * piece)

    def dev(z=z, x=x, y=y, c=c):
        return {"fs": z * 2 + x, "tp": y * 2 + c}

    def rc(src, dst, send, recv, to):
        return pltpu.make_async_remote_copy(
            src_ref=src, dst_ref=dst, send_sem=send, recv_sem=recv, device_id=to, device_id_type=MESH
        )

    def landed(dst, recv):
        pltpu.make_async_remote_copy(
            src_ref=dst, dst_ref=dst, send_sem=recv, recv_sem=recv, device_id=dev(x=1 - x), device_id_type=MESH
        ).wait_recv()

    barrier = pltpu.get_barrier_semaphore()
    peers = [dev(z=pick(TARGETS, k)) for k in range(3)] + [dev(x=1 - x), dev(y=1 - y), dev(c=1 - c)]
    peers.append(dev(y=1 - y, c=1 - c))
    for peer in peers:
        pl.semaphore_signal(barrier, inc=1, device_id=peer, device_id_type=MESH)
    pl.semaphore_wait(barrier, len(peers))

    always, pending = None, []

    def go(copy, condition=always):
        if condition is None:
            copy.start()
        else:
            @pl.when(condition)
            def _():
                copy.start()
        pending.append((copy, condition))

    def pool_block(g, plane, column):
        return pool_full.at[g, pl.ds(pl.multiple_of((plane * 2 + column) * depth, depth), depth), :]

    def pool_to_y(ref, plane, column):
        f = plane * 2 + column
        go(rc(ref, pool_block(me, plane, column), py_s.at[f], py_r.at[f], dev(y=1 - y)))

    def pool_to_x(ref, plane):
        go(rc(ref, pool_block(me, plane, x), px_s.at[plane], px_r.at[plane], dev(x=1 - x)))

    def pool_to_c(g, k):
        go(rc(pool_full.at[g], pool_full.at[g], pc_s.at[k], pc_r.at[k], dev(c=1 - c)))

    own_pool = pool_ref.at[me]
    for k in range(3):
        t = pick(TARGETS, k)
        go(rc(own_pool, pool_block(me, z, x), pz_s.at[t], pz_r.at[z], dev(z=t)))
    pool_to_x(own_pool, z)
    pool_to_y(own_pool, z, x)

    weights = (up_ref, down_ref)
    fulls = (up_full, down_full)

    def slot(stream, plane, p):
        return (stream * nz + plane) * most + p

    def block(stream, plane, column, p):
        return fulls[stream].at[
            pl.ds(p * piece, piece), pl.ds(pl.multiple_of((plane * 2 + column) * cols, cols), cols)
        ]

    def own_piece(stream, plane, p):
        start = pl.multiple_of(base_of(plane) + p * piece, piece)
        return weights[stream].at[pl.ds(start, piece), :]

    def some(p, plane):
        return always if p < min(ENDS, INNER) else p < count_of(plane)

    def spread_z(stream, order):
        for p, k in order:
            t = pick(DTARGETS if stream else TARGETS, k)
            go(
                rc(own_piece(stream, t, p), block(stream, z, x, p), wz_s.at[slot(stream, t, p)],
                   wz_r.at[slot(stream, z, p)], dev(z=t)),
                some(p, t),
            )

    def spread_x(stream, pieces):
        for p in pieces:
            go(
                rc(own_piece(stream, z, p), block(stream, z, x, p), wx_s.at[slot(stream, z, p)],
                   wx_r.at[slot(stream, z, p)], dev(x=1 - x)),
                some(p, z),
            )

    def guarded(condition, body):
        if condition is None:
            body()
        else:
            pl.when(condition)(body)

    def relay(stream, k, pieces):
        s = pick(NEAR, k)
        for p in pieces:
            condition = some(p, z)
            ref = block(stream, s, x, p)
            guarded(condition, lambda ref=ref, p=p: landed(ref, wz_r.at[slot(stream, s, p)]))
            go(rc(ref, ref, wx_s.at[slot(stream, s, p)], wx_r.at[slot(stream, s, p)], dev(x=1 - x)), condition)

    def from_x(stream, s, pieces):
        for p in pieces:
            ref = block(stream, s, 1 - x, p)
            guarded(some(p, z), lambda ref=ref, p=p: landed(ref, wx_r.at[slot(stream, s, p)]))

    every = range(most)
    early = range(most // 2)
    late = range(most // 2, most)
    spread_z(UPS, [(p, k) for p in every for k in range(3)])
    spread_x(UPS, early)

    step = 32 if rows % 32 == 0 else rows

    @pl.loop(0, rows // step)
    def _(i):
        r = pl.ds(pl.multiple_of(i * step, step), step)
        v = tok_ref[r, :].astype(f32)
        v = v * lax.rsqrt(jnp.mean(v * v, axis=-1, keepdims=True) + EPS) * gmix_ref[...]
        v = v.astype(bf)
        ext[pl.ds(pl.multiple_of(HALO + i * step, HALO), step), :] = v.astype(f32)

    edge[0] = ext[rows : rows + HALO, :].astype(bf)
    edge[1] = ext[HALO : 2 * HALO, :].astype(bf)
    for side, (buffer, d) in enumerate(((before, 1), (after, tp - 1))):
        to = {"fs": me_fs, "tp": lax.rem(me + d, tp)}
        go(rc(edge.at[side], buffer, halo_s.at[side], halo_r.at[side], to))

    pool_full[me, pl.ds(pl.multiple_of(me_fs * depth, depth), depth), :] = pool_ref[me, :, :]
    for k in range(3):
        s = pick(NEAR, k)
        ref = pool_block(me, s, x)
        landed(ref, pz_r.at[s])
        pool_to_x(ref, s)
        pool_to_y(ref, s, x)
    spread_x(UPS, late)
    mine = pl.ds(pl.multiple_of(me_fs * cols, cols), cols)
    for stream in (UPS, DOWNS):
        for p in range(most):
            def keep(stream=stream, p=p):
                start = pl.multiple_of(base_of(z) + p * piece, piece)
                fulls[stream][p * piece : (p + 1) * piece, mine] = weights[stream][pl.ds(start, piece), :]
            guarded(some(p, z), keep)
    landed(before, halo_r.at[0])
    landed(after, halo_r.at[1])
    offset = me * rows
    lower_open = (lax.rem(offset, SEQ_LEN) != 0).astype(f32)
    upper_open = (lax.rem(offset + rows, SEQ_LEN) != 0).astype(f32)
    ext[0:HALO, :] = before[...].astype(f32) * lower_open
    ext[rows + HALO : rows + 2 * HALO, :] = after[...].astype(f32) * upper_open
    for k in range(nz):
        s = z if k == 0 else pick(NEAR, k - 1)
        ref = pool_block(me, s, 1 - x)
        landed(ref, px_r.at[s])
        pool_to_y(ref, s, 1 - x)
    pool_to_c(me, 0)
    peer_c, peer_y, peer_yc = y * 2 + 1 - c, (1 - y) * 2 + c, (1 - y) * 2 + 1 - c
    for f in range(2 * nz):
        landed(pool_block(peer_y, f // 2, f % 2), py_r.at[f])
    pool_to_c(peer_y, 1)
    landed(pool_full.at[peer_c], pc_r.at[0])
    landed(pool_full.at[peer_yc], pc_r.at[1])

    def rows_of(s, t):
        return pl.ds(pl.multiple_of(s * seq + t * rows, rows), rows)

    my_rows = rows_of(q, me)
    position = lax.rem(offset + lax.broadcasted_iota(jnp.int32, (rows, 1), 0), SEQ_LEN)
    for index, reach in enumerate(WINDOWS):
        half = reach // 2
        g = slice(index * group, (index + 1) * group)
        level = ext[:, g]
        own = level[HALO : HALO + rows]
        shift = 1
        while shift < reach:
            level = level + pltpu.roll(level, shift, 0)
            shift *= 2
        if half > 1:
            level = pltpu.roll(level, rows + 2 * HALO - (half - 1), 0)
        window = level[HALO : HALO + rows]
        counts = (jnp.minimum(position + half, SEQ_LEN) - jnp.maximum(position - half, 0)).astype(f32)
        pooled = (window / counts - own).astype(bf)
        mixed = jnp.dot(pooled, pool_full[index], preferred_element_type=f32)
        first_all[my_rows, g] = (tok_ref[:, g].astype(f32) + mixed * scale_ref[:, g]).astype(bf)

    part_rows = rows // HALVES

    def first_part(s, t, h):
        return first_all.at[pl.ds(pl.multiple_of(s * seq + t * rows + h * part_rows, part_rows), part_rows), :]

    def share(s, t, k, to, h):
        ref = first_part(s, t, h)
        go(rc(ref, ref, f_s.at[k * HALVES + h], f_r.at[k * HALVES + h], to))

    def shared(s, t, k, h):
        landed(first_part(s, t, h), f_r.at[k * HALVES + h])

    halves = range(HALVES)
    for h in halves:
        share(q, me, 0, dev(z=zp), h)
        share(q, me, 1, dev(y=1 - y), h)
        share(q, me, 3, dev(c=1 - c), h)

    def groups(s, yy):
        return s * seq + yy * 2 * rows

    def norm(begin):
        @pl.loop(0, 2 * rows // step)
        def _(i):
            r = pl.ds(pl.multiple_of(begin + i * step, step), step)
            v = first_all[r, :].astype(f32)
            v = v * lax.rsqrt(jnp.mean(v * v, axis=-1, keepdims=True) + EPS) * gmlp_ref[...]
            inner_all[r, :] = v.astype(bf)

    def up(begin, lo, hi):
        g = pl.ds(pl.multiple_of(begin, 2 * rows), 2 * rows)

        @pl.loop(lo, hi)
        def _(j):
            h = pl.ds(pl.multiple_of(j * piece, piece), piece)
            pre = lax.dot_general(
                inner_all[g, :], up_full[h, :], (((1,), (1,)), ((), ())), preferred_element_type=f32
            )
            hidden[g, h] = jnp.square(jnp.maximum(pre, 0.0)).astype(bf)

    def pull(pieces):
        for p in pieces:
            for k in range(3):
                relay(UPS, k, (p,))

    def ready(pieces):
        for s in range(nz):
            from_x(UPS, s, pieces)

    def forward_z():
        for h in halves:
            shared(1 - q, me, 0, h)
            share(1 - q, me, 2, dev(y=1 - y), h)
            share(1 - q, me, 4, dev(c=1 - c), h)

    def forward_y(s, k, kc):
        for h in halves:
            shared(s, peer_y, k, h)
            share(s, peer_y, kc, dev(c=1 - c), h)

    def from_c(s, t, k):
        for h in halves:
            shared(s, t, k, h)

    g0, g1, g2, g3 = groups(q, y), groups(q, 1 - y), groups(1 - q, y), groups(1 - q, 1 - y)
    quarter = most // 4
    p0, p1, p2, p3 = [range(k * quarter, most if k == 3 else (k + 1) * quarter) for k in range(4)]
    half = 2 * quarter
    pull(p0)
    from_c(q, peer_c, 3)
    norm(g0)
    pull(p1)
    ready(p0)
    ready(p1)
    up(g0, 0, half)
    spread_x(DOWNS, every)
    forward_y(q, 1, 5)
    from_c(q, peer_yc, 5)
    norm(g1)
    up(g1, 0, half)
    pull(p2)
    spread_z(DOWNS, [(p, k) for k in range(3) for p in every])
    pull(p3)
    forward_z()
    from_c(1 - q, peer_c, 4)
    norm(g2)
    up(g2, 0, half)
    ready(p2)
    relay(DOWNS, 0, every)
    ready(p3)
    up(g0, half, count_of(z))
    up(g1, half, count_of(z))
    up(g2, half, count_of(z))
    forward_y(1 - q, 2, 6)
    from_c(1 - q, peer_yc, 6)
    norm(g3)
    up(g3, 0, count_of(z))
    first_sends = list(pending)
    pending.clear()

    chunk = 2 * rows
    orow = pl.ds(pl.multiple_of(q * seq, seq), seq)
    prow = pl.ds(pl.multiple_of((1 - q) * seq, seq), seq)
    fine = 128

    def unit(i, j):
        plane = jnp.where(z < 2, i, nz - 1 - i)
        column = x if j == 0 else 1 - x
        return plane, column, (i // 2) * 2 + j, i * 2 + j

    def each(begin, size, body):
        @pl.loop(0, size // fine)
        def _(i):
            body(pl.ds(pl.multiple_of(begin + i * fine, fine), fine), pl.ds(pl.multiple_of(i * fine, fine), fine))

    def send_part(i, j):
        plane, column, s, u = unit(i, j)
        go(rc(part_send.at[s], part_recv.at[s], d_s.at[u], d_r.at[u], dev(c=1 - c)), lax.rem(plane, 2) != c)

    def multiply(theirs, deep, cc, slots):
        def all_rows(theirs, deep):
            @pl.loop(0, 2 * seq // chunk)
            def _(k):
                r = pl.ds(pl.multiple_of(k * chunk, chunk), chunk)
                value = jnp.dot(hidden[r, 0:deep], down_full[0:deep, cc], preferred_element_type=f32)
                for n, s in enumerate(slots):
                    lane = slice(n * cols, (n + 1) * cols)
                    if theirs:
                        part_send[s, r, :] = value[:, lane].astype(bf)
                    else:
                        part[s, r, :] = value[:, lane]

        pl.when(theirs)(lambda: all_rows(True, deep))
        pl.when(jnp.logical_not(theirs))(lambda: all_rows(False, deep))

    def by_depth(body):
        if ENDS == INNER:
            body(ENDS * piece)
        else:
            pl.when(is_end(z))(lambda: body(ENDS * piece))
            pl.when(jnp.logical_not(is_end(z)))(lambda: body(INNER * piece))

    def product(i, j):
        plane, column, s, u = unit(i, j)
        cc = pl.ds(pl.multiple_of((plane * 2 + column) * cols, cols), cols)
        if j == 1:
            from_x(DOWNS, plane, every)
        by_depth(lambda deep: multiply(lax.rem(plane, 2) != c, deep, cc, (s,)))
        send_part(i, j)

    def wide_product(i):
        plane = jnp.where(z < 2, i, nz - 1 - i)
        cc = pl.ds(pl.multiple_of(plane * 2 * cols, 2 * cols), 2 * cols)
        from_x(DOWNS, plane, every)
        slots = ((i // 2) * 2 + x, (i // 2) * 2 + 1 - x)
        by_depth(lambda deep: multiply(lax.rem(plane, 2) != c, deep, cc, slots))
        for j in (0, 1):
            send_part(i, j)

    def stage1(i, j):
        plane, column, s, u = unit(i, j)
        ours = lax.rem(plane, 2) == c
        home = lax.div(plane, 2) == y

        def fold(begin, size, keep):
            def body(r, _):
                value = part[s, r, :] + part_recv[s, r, :].astype(f32)
                if keep:
                    part[s, r, :] = value
                else:
                    part_recv[s, r, :] = value.astype(bf)
            each(begin, size, body)

        @pl.when(ours)
        def _():
            landed(part_recv.at[s], d_r.at[u])
            if not Y_FIRST[i][j]:
                fold((1 - q) * seq, seq, False)

        if Y_FIRST[i][j]:
            pl.when(ours & home)(lambda: fold(0, 2 * seq, True))
            pl.when(ours & jnp.logical_not(home))(lambda: fold(0, 2 * seq, False))
            go(rc(part_recv.at[s], y_recv.at[j], y_s.at[u], y_r.at[u], dev(y=1 - y)), ours & jnp.logical_not(home))
        else:
            go(rc(part_recv.at[s, prow, :], z_recv.at[s], z_s.at[u], z_r.at[u], dev(z=zp)), ours)
            pl.when(ours)(lambda: fold(q * seq, seq, True))

    def stage2(i, j):
        plane, column, s, u = unit(i, j)
        ours = lax.rem(plane, 2) == c
        home = lax.div(plane, 2) == y
        if Y_FIRST[i][j]:
            @pl.when(ours & home)
            def _():
                landed(y_recv.at[j], y_r.at[u])

                def out(r, _):
                    y_recv[j, r, :] = (part[s, r, :] + y_recv[j, r, :].astype(f32)).astype(bf)
                each((1 - q) * seq, seq, out)

            go(rc(y_recv.at[j, prow, :], z_recv.at[s], z_s.at[u], z_r.at[u], dev(z=zp)), ours & home)

            @pl.when(ours & home)
            def _():
                def kept(r, _):
                    part[s, r, :] = part[s, r, :] + y_recv[j, r, :].astype(f32)
                each(q * seq, seq, kept)
        else:
            @pl.when(ours)
            def _():
                landed(z_recv.at[s], z_r.at[u])

            @pl.when(ours & jnp.logical_not(home))
            def _():
                def out(r, l):
                    part_recv[s, r, :] = (part[s, r, :] + z_recv[s, l, :].astype(f32)).astype(bf)
                each(q * seq, seq, out)

            go(rc(part_recv.at[s, orow, :], y_recv.at[j, orow, :], y_s.at[u], y_r.at[u], dev(y=1 - y)),
               ours & jnp.logical_not(home))

            @pl.when(ours & home)
            def _():
                def kept(r, l):
                    part[s, r, :] = part[s, r, :] + z_recv[s, l, :].astype(f32)
                each(q * seq, seq, kept)

    def stage3(i, j):
        plane, column, s, u = unit(i, j)

        @pl.when(plane == me)
        def _():
            if Y_FIRST[i][j]:
                landed(z_recv.at[s], z_r.at[u])
            else:
                landed(y_recv.at[j, orow, :], y_r.at[u])
            here = pl.ds(pl.multiple_of(column * cols, cols), cols)
            cc = pl.ds(pl.multiple_of(me * own_cols + column * cols, cols), cols)

            def body(r, l):
                more = z_recv[s, l, :] if Y_FIRST[i][j] else y_recv[j, r, :]
                value = part[s, r, :] + more.astype(f32) + first_all[r, cc].astype(f32)
                total[l, here] = value
                square = value * value
                lump = square[:, 0:128]
                for k in range(1, cols // 128):
                    lump = lump + square[:, k * 128 : (k + 1) * 128]
                stat[l, :] = stat[l, :] + lump
            each(q * seq, seq, body)

    stat[...] = jnp.zeros_like(stat)
    both = (0, 1)

    def run(body, i):
        for j in both:
            body(i, j)

    def drain():
        for copy, condition in pending:
            guarded(condition, copy.wait_send)
        pending.clear()

    wide_product(0)
    relay(DOWNS, 1, every)
    wide_product(1)
    run(stage1, 0)
    run(stage1, 1)
    wide_product(2)
    run(stage1, 2)
    relay(DOWNS, 2, every)
    run(product, 3)
    run(stage2, 1)
    run(stage1, 3)
    for copy, condition in first_sends:
        guarded(condition, copy.wait_send)
    run(stage2, 0)
    run(stage2, 2)
    run(stage2, 3)
    run(stage3, 0)
    run(stage3, 1)
    run(stage3, 2)
    run(stage3, 3)

    turned = jnp.transpose(stat[...])
    stat_out[...] = jnp.broadcast_to(jnp.sum(turned, axis=0, keepdims=True), stat_out.shape)
    for d in range(1, tp):
        to = {"fs": me_fs, "tp": lax.rem(me + d, tp)}
        go(rc(stat_out, stat_in.at[d], st_s.at[d], st_r.at[d], to))
    drain()
    squares = stat_out[...]
    for d in range(1, tp):
        landed(stat_in.at[d], st_r.at[d])
        squares = squares + stat_in[d]
    factor = lax.rsqrt(squares / width + EPS)
    stat[...] = jnp.transpose(jnp.broadcast_to(factor[0:1], (128, seq)))

    @pl.loop(0, seq // 128)
    def _(i):
        r = pl.ds(pl.multiple_of(i * 128, 128), 128)
        out_ref[r, :] = (total[r, :] * stat[r, 0:1] * gout_ref[...]).astype(bf)


def plane_local(tokens, pool_weight, pool_scale, gain_mix, gain_mlp, w_up, w_down, gain_out):
    n, tp = lax.axis_size("fs"), lax.axis_size("tp")
    rows, width = tokens.shape
    hid, cols = w_up.shape
    seq, own = rows * tp, width // tp
    bf, f32 = jnp.bfloat16, jnp.float32
    vmem = pl.BlockSpec(memory_space=pltpu.VMEM)
    dma = pltpu.SemaphoreType.DMA
    most = max(ENDS, INNER)
    deep = hid // (ENDS + INNER) * most
    lots = 2 * 4 * most
    return pl.pallas_call(
        plane_kernel,
        out_shape=jax.ShapeDtypeStruct((seq, own), bf),
        in_specs=[vmem] * 8,
        out_specs=vmem,
        scratch_shapes=[
            pltpu.VMEM((pool_weight.shape[0], pool_weight.shape[1] * n, pool_weight.shape[2]), bf),
            pltpu.VMEM((deep, width), bf),
            pltpu.VMEM((deep, width), bf),
            pltpu.VMEM((rows + 2 * HALO, width), f32),
            pltpu.VMEM((2 * seq, width), bf),
            pltpu.VMEM((2 * seq, width), bf),
            pltpu.VMEM((2 * seq, deep), bf),
            pltpu.VMEM((4, 2 * seq, cols), bf),
            pltpu.VMEM((4, 2 * seq, cols), bf),
            pltpu.VMEM((4, 2 * seq, cols), f32),
            pltpu.VMEM((2, 2 * seq, cols), bf),
            pltpu.VMEM((4, seq, cols), bf),
            pltpu.VMEM((HALO, width), bf),
            pltpu.VMEM((HALO, width), bf),
            pltpu.VMEM((2, HALO, width), bf),
            pltpu.VMEM((seq, own), f32),
            pltpu.VMEM((seq, 128), f32),
            pltpu.VMEM((8, seq), f32),
            pltpu.VMEM((tp, 8, seq), f32),
            dma((4,)), dma((4,)), dma((4,)), dma((4,)), dma((8,)), dma((8,)), dma((2,)), dma((2,)),
            dma((lots,)), dma((lots,)), dma((lots,)), dma((lots,)),
            dma((2,)), dma((2,)),
            dma((7 * HALVES,)), dma((7 * HALVES,)),
            dma((8,)), dma((8,)), dma((8,)), dma((8,)), dma((8,)), dma((8,)),
            dma((tp,)), dma((tp,)),
        ],
        compiler_params=pltpu.CompilerParams(
            collective_id=0, has_side_effects=True, vmem_limit_bytes=63 * 1024 * 1024
        ),
    )(
        tokens, pool_weight, w_up, w_down,
        pool_scale.reshape(1, -1), gain_mix.reshape(1, -1), gain_mlp.reshape(1, -1),
        gain_out.reshape(1, -1),
    )


def grid_width(mesh):
    n = mesh.shape["fs"]
    try:
        line = mesh.devices.reshape(n, -1)[:, 0]
        nx = len({d.coords[0] for d in line})
        if n % nx == 0:
            return nx
    except AttributeError:
        pass
    return 2 if n % 2 == 0 else 1


def solution(mesh):
    n, tp, nx = mesh.shape["fs"], mesh.shape["tp"], grid_width(mesh)
    if nx == 2 and n == 8 and tp == 4:
        body = plane_local
    else:
        body = functools.partial(ring_local, ring_order(n, nx))
    return jax.shard_map(
        body,
        mesh=mesh,
        in_specs=(
            P(("fs", "tp"), None),
            P(None, "fs", None),
            P(),
            P(),
            P(),
            P("tp", "fs"),
            P("tp", "fs"),
            P("tp"),
        ),
        out_specs=P("fs", "tp"),
        check_vma=False,
    )
```
